512 devices in a mesh: sp: 32 (over z, core), tp: 16 (over y, x).
Axes of the slice: x: 4, y: 4, z: 16, core: 2. Of those that a mesh axis runs over, the one named last changes fastest.
Arguments:
- tokens: bfloat16 [24576, 2048], P('sp', 'tp'), may hold values from -26 to 26, as said below
- mix_gain: bfloat16 [2, 2048], replicated, may hold values from 0.099609375 to 1.8984375
- x_weight: bfloat16 [2, 2048, 1024], P(None, 'sp', 'tp'), may hold values from -0.125 to 0.125
- gate_weight: bfloat16 [2, 2048, 1024], P(None, 'sp', 'tp'), may hold values from -0.125 to 0.125
- conv_taps: bfloat16 [2, 4, 1024], P(None, None, 'tp'), may hold values from -3 to 3
- a_maps: bfloat16 [2, 16, 64, 64], P(None, 'tp'), may hold values from -0.75 to 0.75
- i_maps: bfloat16 [2, 16, 64, 64], P(None, 'tp'), may hold values from -0.75 to 0.75
- decay_rate: float32 [2, 1024], P(None, 'tp'), as said below
- pace: float32 [24576], P('sp'), may hold values from 0.35 to 2.8, as said below
- jumps: float32 [24576], P('sp'), may hold values from -0.7 to 0, as said below
- out_gain: bfloat16 [2, 1024], P(None, 'tp'), may hold values from 0.099609375 to 1.8984375
- out_weight: bfloat16 [2, 1024, 2048], P(None, 'sp', 'tp'), may hold values from -0.1875 to 0.1875
Outputs:
- stream: bfloat16 [24576, 2048], P('sp', 'tp')
The draws below stay inside these ranges and needn't reach their ends.
Inputs may be any that keep to these rules, and one draw needn't show every extreme that they name: `tokens`: random-looking real values; feature scales differ along the features. `decay_rate`: positive. `pace`: positive. `jumps`: zero or negative.
All inputs are finite; a program needn't handle non-finite values.
Results may differ from the reference program's by a relative error of at most 0.01.
Values may be sent and summed in bfloat16 or wider, within the bound.
A program may use at most 64 MiB of HBM per device.

```python
import math
import jax
import jax.numpy as jnp
from jax import lax

D = 2048
D_REC = 1024
HEAD = 64
WIDTH = 4
LAYERS = 2
TOK_DEV = 768
TOKENS = 24576
HEADS = 16


def draw_tokens(key, part):
    first = jax.random.fold_in(key, 11)
    second = jax.random.fold_in(key, 12)
    ramp = jnp.exp(jnp.linspace(0.0, math.log(3.0), D)).astype(jnp.float32)
    rough = jnp.exp(jax.random.uniform(second, (D,), jnp.float32, -0.35, 0.35))
    values = jnp.clip(jax.random.normal(first, (TOKENS, D), jnp.float32), -6.0, 6.0)
    return (values * ramp[None, :] * rough[None, :]).astype(jnp.bfloat16)


def draw_decay_rate(key, part):
    first = jax.random.fold_in(key, 21)
    second = jax.random.fold_in(key, 22)
    third = jax.random.fold_in(key, 23)
    share = 0.5
    fast = jax.random.uniform(first, (LAYERS, D_REC), jnp.float32) < share
    quick = jnp.exp(jax.random.uniform(second, (LAYERS, D_REC), jnp.float32, math.log(0.004), math.log(0.012)))
    slow = jnp.exp(jax.random.uniform(third, (LAYERS, D_REC), jnp.float32, math.log(0.02), math.log(0.1))) / TOKENS
    return jnp.where(fast, quick, slow).astype(jnp.float32)


def draw_pace(key, part):
    first = jax.random.fold_in(key, 31)
    second = jax.random.fold_in(key, 32)
    blocks = TOKENS // TOK_DEV
    block_factor = jnp.exp(jax.random.uniform(first, (blocks,), jnp.float32, math.log(0.5), math.log(2.0)))
    fine = jnp.exp(jax.random.uniform(second, (TOKENS,), jnp.float32, math.log(0.7), math.log(1.4)))
    return (jnp.repeat(block_factor, TOK_DEV) * fine).astype(jnp.float32)


def draw_jumps(key, part):
    first = jax.random.fold_in(key, 41)
    second = jax.random.fold_in(key, 42)
    spots = jax.random.randint(first, (6,), 0, TOKENS)
    sizes = jnp.log(jax.random.uniform(second, (6,), jnp.float32, 0.5, 0.8))
    return jnp.zeros((TOKENS,), jnp.float32).at[spots].set(sizes)


def levels(rng, shape, cuts, smallest, top_value):
    loudness = 1.0
    for position, parts in cuts:
        heights = jax.random.uniform(jax.random.fold_in(jax.random.fold_in(rng, 6), position), (parts,), jnp.float32, smallest / len(cuts), top_value / len(cuts))
        loudness = loudness * jnp.repeat(jnp.exp(heights), shape[position] // parts).reshape((-1,) + (1,) * (len(shape) - 1 - position))
    return loudness


def normal_values(stream_key, extent, deviation, limit, split=(), held_as=jnp.bfloat16):
    result = jax.random.normal(stream_key, extent, jnp.float32) * deviation
    if len(split) > 0:
        result = levels(stream_key, extent, split, -0.22, 0.18) * result
    return jnp.clip(result, min=-limit, max=limit).astype(held_as)


def setup_inputs(seed: int = 0) -> dict:
    seeds = jax.random.split(jax.random.key(seed), 13)
    return {
        "tokens": draw_tokens(jax.random.fold_in(seeds[12], 71), 0),
        "mix_gain": jnp.clip(1.0 + 0.18 * jax.random.normal(seeds[1], (LAYERS, D), jnp.float32), 0.099609375, 1.8984375).astype(jnp.bfloat16),
        "x_weight": normal_values(seeds[2], (LAYERS, D, D_REC), D ** -0.5, 0.125, ((1, 32), (2, 16))),
        "gate_weight": normal_values(seeds[3], (LAYERS, D, D_REC), D ** -0.5, 0.125, ((1, 32), (2, 16))),
        "conv_taps": normal_values(seeds[4], (LAYERS, WIDTH, D_REC), WIDTH ** -0.5, 3.0, ((2, 16),)),
        "a_maps": normal_values(seeds[5], (LAYERS, HEADS, HEAD, HEAD), HEAD ** -0.5, 0.75, ((1, 16),)),
        "i_maps": normal_values(seeds[6], (LAYERS, HEADS, HEAD, HEAD), HEAD ** -0.5, 0.75, ((1, 16),)),
        "decay_rate": draw_decay_rate(jax.random.fold_in(seeds[12], 71), 0),
        "pace": draw_pace(jax.random.fold_in(seeds[12], 71), 0),
        "jumps": draw_jumps(jax.random.fold_in(seeds[12], 71), 0),
        "out_gain": jnp.clip(1.0 + 0.18 * jax.random.normal(seeds[10], (LAYERS, D_REC), jnp.float32), 0.099609375, 1.8984375).astype(jnp.bfloat16),
        "out_weight": normal_values(seeds[11], (LAYERS, D_REC, D), D_REC ** -0.5, 0.1875, ((1, 32), (2, 16))),
    }


EPS = 1e-06
GATE_C = 8.0

def combine(first, second):
    return (first[0] * second[0], second[0] * first[1] + second[1])

def reference(tokens, mix_gain, x_weight, gate_weight, conv_taps, a_maps, i_maps, decay_rate, pace, jumps, out_gain, out_weight):
    f32 = jnp.float32
    stream = tokens
    for layer in range(LAYERS):
        xf = stream.astype(f32)
        normed = (xf * lax.rsqrt(lax.optimization_barrier(jnp.mean(xf * xf, axis=1, keepdims=True)) + EPS) * mix_gain[layer].astype(f32)).astype(jnp.bfloat16)
        xr = jnp.dot(normed, x_weight[layer], preferred_element_type=f32).astype(jnp.bfloat16)
        gr = jnp.dot(normed, gate_weight[layer], preferred_element_type=f32).astype(jnp.bfloat16)
        padded = jnp.pad(xr, ((WIDTH - 1, 0), (0, 0))).astype(f32)
        taps = conv_taps[layer].astype(f32)
        conv = jnp.zeros((TOKENS, D_REC), f32)
        for k in range(WIDTH):
            conv = conv + taps[k][None, :] * padded[k:k + TOKENS]
        xc = conv.astype(jnp.bfloat16)
        grouped = xc.astype(f32).reshape(TOKENS, HEADS, HEAD)
        rgate = jax.nn.sigmoid(jnp.einsum('thi,hij->thj', grouped, a_maps[layer].astype(f32)).reshape(TOKENS, D_REC))
        igate = jax.nn.sigmoid(jnp.einsum('thi,hij->thj', grouped, i_maps[layer].astype(f32)).reshape(TOKENS, D_REC))
        log_a = -GATE_C * rgate * decay_rate[layer][None, :] * pace[:, None] + jumps[:, None]
        decay = jnp.exp(log_a)
        drive = jnp.sqrt(-jnp.expm1(2.0 * log_a)) * igate * xc.astype(f32)
        _, state = lax.associative_scan(combine, (decay, drive), axis=0)
        rec = state * jax.nn.gelu(gr.astype(f32))
        scale = lax.rsqrt(lax.optimization_barrier(jnp.mean(rec * rec, axis=1, keepdims=True)) + EPS)
        mixed = (rec * out_gain[layer].astype(f32)[None, :]).astype(jnp.bfloat16)
        stream = (xf + jnp.dot(mixed, out_weight[layer], preferred_element_type=f32) * scale).astype(jnp.bfloat16)
    return stream
```

```python
import functools

import jax
import jax.numpy as jnp
from jax import lax
from jax.experimental import pallas as pl
from jax.experimental.pallas import tpu as pltpu
from jax.sharding import PartitionSpec as P

HEAD = 64
WIDTH = 4
LAYERS = 2
EPS = 1e-06
GATE_C = 8.0
RIM = 16
LANE = 128
ROWS = 8

f32 = jnp.float32
bf16 = jnp.bfloat16


def swapped(x):
    return pltpu.roll(x, HEAD, 1)


def lower_half(shape):
    return lax.broadcasted_iota(jnp.int32, shape, len(shape) - 1) < HEAD


def halves(first, second):
    return jnp.where(lower_half(first.shape), first, second)


def chained(first, second):
    low = lower_half(second.shape)
    return jnp.where(low, second, swapped(second)) * first + jnp.where(low, 0.0, second)


def gelu(x):
    return 0.5 * x * (1.0 + jnp.tanh(0.7978845608028654 * (x + 0.044715 * (x * x * x))))


def one_minus_exp(y, decay):
    series = jnp.ones_like(y)
    for k in range(8, 1, -1):
        series = 1.0 - (y * (1.0 / k)) * series
    return jnp.where(y < 0.5, y * series, 1.0 - decay * decay)


def kernel(n, tq, tok, gain, wxg, wo, maps, small, pj, out,
           WX, WO, MAPS, SMALL, XM, XH, NRM, XR, GEL, BD, PAR, AS, BS, LOC, ACU, MIX, MX,
           PO, PR, ZO, ZR, FS, OB, send, recv):
    nt, nz, ns = n * n, n * n, 2 * n * n
    C = n * HEAD
    pairs = n // 2
    D = nt * LANE
    steps = tq // ROWS
    s, tp = lax.axis_index("sp"), lax.axis_index("tp")
    c, z = s % 2, s // 2
    a, b = z // n, z % n
    y, x = tp // n, tp % n
    p, q = x + c * (y - x), y + c * (x - y)

    def tp_of(core, pp, qq):
        return (qq * n + pp) + core * ((pp * n + qq) - (qq * n + pp))

    sent = []
    numbers = iter(range(10000))

    def put(src, dst, sp_to, tp_to, slot=None):
        slot = next(numbers) if slot is None else slot
        cp = pltpu.make_async_remote_copy(
            src_ref=src, dst_ref=dst, send_sem=send, recv_sem=recv.at[slot],
            device_id={"sp": sp_to, "tp": tp_to}, device_id_type=pl.DeviceIdType.MESH)
        cp.start()
        sent.append(cp)
        return cp

    def landed(copies):
        for cp in copies:
            cp.wait_recv()

    def landed_all(ref, slot):
        pltpu.make_async_copy(ref, ref, recv.at[slot]).wait()

    near = range(1, n)

    def z1_x(l):
        return [put(wxg.at[l], WX.at[l, p, a, b, c], (((a + d) % n) * n + b) * 2 + c, tp) for d in near]

    i0, i1 = a + c * (b - a), b + c * (a - b)

    def z1_o(l):
        return [put(wo.at[l], WO.at[l, p, i0, i1, c], (((a + d) % n) * n + b) * 2 + c, tp) for d in near]

    def z2_x(l):
        ref = WX.at[l, p, :, b, c]
        return [put(ref, ref, (a * n + (b + d) % n) * 2 + c, tp) for d in near]

    def z2_o(l):
        made = []
        for d in near:
            for k in range(n):
                ref = WO.at[l, p, k + c * (b - k), b + c * (k - b), c]
                made.append(put(ref, ref, (a * n + (b + d) % n) * 2 + c, tp))
        return made

    def twin_x(l):
        return [put(WX.at[l, p, :, :, c], WX.at[l, q, :, :, c], z * 2 + 1 - c, tp)]

    def twin_o(l):
        return [put(WO.at[l, p, k, :, c], WO.at[l, q, :, k, c], z * 2 + 1 - c, tp) for k in range(n)]

    def across(ref):
        return [put(ref, ref, s, tp_of(c, (p + d) % n, q)) for d in near]

    own = pl.ds(pl.multiple_of(p * tq, tq), tq)
    t_a = []
    for d in near:
        pp = (p + d) % n
        rows = pl.ds(pl.multiple_of(pp * tq, tq), tq)
        t_a.append(put(tok.at[rows], XM.at[0, tp], s, tp_of(c, pp, q)))
    rim0 = next(numbers)
    rim_sends = []
    for k in range(n):
        e, pp = (k + 1) // n, (k + 1) % n
        src = tok.at[(k + 1) * tq - RIM:(k + 1) * tq]
        for qq in range(n):
            cp = pltpu.make_async_remote_copy(
                src_ref=src, dst_ref=XH.at[0, tp], send_sem=send, recv_sem=recv.at[rim0],
                device_id={"sp": (s + e) % ns, "tp": tp_of((c + e) % 2, pp, qq)},
                device_id_type=pl.DeviceIdType.MESH)
            if e:
                cp.start()
                sent.append(cp)
            else:
                mine = (1 - jnp.minimum(abs(pp - p), 1)) * (1 - jnp.minimum(abs(qq - q), 1))

                @pl.when(mine == 0)
                def _():
                    cp.start()

                @pl.when(mine == 1)
                def _():
                    XH[0, tp] = src[...]
                rim_sends.append((cp, mine))
    wx = [z1_x(0), None]
    wout = [z1_o(0), None]
    m_in = [put(maps, MAPS.at[p], s, tp_of(c, (p + d) % n, q)) for d in near]
    s_in = [put(small, SMALL.at[tp], s, (tp + d) % nt) for d in range(1, nt)]
    wx[1], wout[1] = z1_x(1), z1_o(1)

    XM[0, tp] = tok[own]
    for l in range(LAYERS):
        WX[l, p, a, b, c] = wxg[l]
        WO[l, p, i0, i1, c] = wo[l]
    MAPS[p] = maps[...]
    SMALL[tp] = small[...]

    landed(t_a)
    t_b = []
    for d in near:
        to = tp_of(c, p, (q + d) % n)
        t_b.append(put(tok.at[own], XM.at[0, tp], s, to))
        for e in near:
            ref = XM.at[0, tp_of(c, (p + e) % n, q)]
            t_b.append(put(ref, ref, s, to))

    landed(wx[0])
    wx[0] = z2_x(0)
    landed(wout[0])
    wout[0] = z2_o(0)

    landed(m_in)
    landed(s_in)
    for l in range(LAYERS):
        for jp in range(pairs):
            even = MAPS[2 * jp, l].astype(f32)
            odd = MAPS[2 * jp + 1, l].astype(f32)
            low = lower_half(even.shape)
            BD[l, jp, :HEAD, :LANE] = jnp.where(low, even, 0.0).astype(bf16)
            BD[l, jp, :HEAD, LANE:] = jnp.where(low, swapped(even), 0.0).astype(bf16)
            BD[l, jp, HEAD:, :LANE] = jnp.where(low, 0.0, swapped(odd)).astype(bf16)
            BD[l, jp, HEAD:, LANE:] = jnp.where(low, 0.0, odd).astype(bf16)
            for qq in range(n):
                PAR[l, qq, jp] = halves(SMALL[tp_of(c, 2 * jp, qq), l], SMALL[tp_of(c, 2 * jp + 1, qq), l])

    def norm_rows(l, block, row):
        total = jnp.zeros((RIM, LANE), f32)
        for t in range(nt):
            v = block(t).astype(f32)
            total = total + v * v
        r = lax.rsqrt(jnp.sum(total, axis=1, keepdims=True) * (1.0 / D) + EPS)
        for t in range(nt):
            cols = slice(t * LANE, (t + 1) * LANE)
            g = gain[l:l + 1, cols].astype(f32)
            NRM[pl.ds(row, RIM), cols] = (block(t).astype(f32) * r * g).astype(bf16)

    def norm(l):
        norm_rows(l, lambda t: XH[l, t], 0)

        @pl.loop(0, tq // RIM)
        def _(i):
            row = pl.multiple_of(i * RIM, RIM)
            norm_rows(l, lambda t: XM[l, t, pl.ds(row, RIM), :], pl.multiple_of(row + RIM, RIM))

    def first_half(l):
        keep = jnp.minimum(s + p, 1).astype(f32)
        normed = NRM[...]
        pace = pj[own, 0:1]
        jump = pj[own, 1:2]
        for jp in range(pairs):
            w = jnp.concatenate(
                [WX[l, 2 * jp].reshape(D, LANE), WX[l, 2 * jp + 1].reshape(D, LANE)], axis=1)
            pr = jnp.dot(normed, w, preferred_element_type=f32).astype(bf16).astype(f32)
            left, right = pr[:, :LANE], pr[:, LANE:]
            xr = halves(left, swapped(right))
            XR[jp, :RIM] = xr[:RIM] * keep
            XR[jp, RIM:] = xr[RIM:]
            GEL[jp] = gelu(halves(swapped(left), right)[RIM:])
            par = PAR[l, q, jp]
            conv = jnp.zeros((tq, LANE), f32)
            for k in range(WIDTH):
                conv = conv + par[k:k + 1] * XR[jp, pl.ds(RIM - WIDTH + 1 + k, tq), :]
            xc = conv.astype(bf16)
            gates = jnp.dot(xc, BD[l, jp], preferred_element_type=f32)
            r = jax.nn.sigmoid(gates[:, :LANE])
            gin = jax.nn.sigmoid(gates[:, LANE:])
            log_a = -GATE_C * r * par[4:5] * pace + jump
            decay = jnp.exp(log_a)
            AS[jp] = decay
            BS[jp] = jnp.sqrt(one_minus_exp(-2.0 * log_a, decay)) * gin * xc.astype(f32)
        starts = []
        for jp in range(pairs):
            run = h = None
            for k in range(steps):
                ak = AS[jp, pl.ds(k, ROWS, stride=steps), :]
                bk = BS[jp, pl.ds(k, ROWS, stride=steps), :]
                h = bk if k == 0 else ak * h + bk
                run = ak if k == 0 else ak * run
                LOC[jp, k], ACU[jp, k] = h, run
            row = lax.broadcasted_iota(jnp.int32, (ROWS, LANE), 0)
            for d in (1, 2, 4):
                before = row >= d
                h = run * jnp.where(before, pltpu.roll(h, d, 0), 0.0) + h
                run = run * jnp.where(before, pltpu.roll(run, d, 0), 1.0)
            av, sv = run[ROWS - 1:], h[ROWS - 1:]
            PO[l, 2 * jp] = halves(av, swapped(sv))
            PO[l, 2 * jp + 1] = halves(swapped(av), sv)
            starts.append((jnp.where(row >= 1, pltpu.roll(run, 1, 0), 1.0),
                           jnp.where(row >= 1, pltpu.roll(h, 1, 0), 0.0)))
        return starts

    def prefix(l):
        made = []
        for d in near:
            made.append(put(PO.at[l], PR.at[l, c, p], s, tp_of(c, (p + d) % n, q)))
        slot = next(numbers)
        for k in range(n):
            for pp in range(n):
                put(PO.at[l, k], PR.at[l, c, p, q], z * 2 + 1 - c, tp_of(1 - c, pp, k), slot)
        for j in range(n):
            PR[l, c, p, j] = PO[l, j]
        landed(made)
        landed_all(PR.at[l, 1 - c], slot)
        identity = jnp.where(lower_half((n, LANE)), 1.0, 0.0)
        total = within = identity
        mine = c * n + p
        for i in range(2 * n):
            piece = jnp.concatenate([PR[l, i // n, i % n, j] for j in range(n)], axis=0)
            within = jnp.where(i < mine, chained(within, piece), within)
            total = chained(total, piece)
        for j in range(n):
            ZO[l, j] = total[j:j + 1]
        slot = next(numbers)
        for d in range(1, nz):
            put(ZO.at[l], ZR.at[l, d - 1], ((z + d) % nz) * 2 + c, tp, slot)
        landed_all(ZR.at[l], slot)
        before = identity
        for d in range(nz - 1, 0, -1):
            piece = jnp.concatenate([ZR[l, d - 1, j] for j in range(n)], axis=0)
            before = jnp.where(d <= z, chained(before, piece), before)
        return chained(before, within)

    def second_half(l, starts, incoming):
        turned = swapped(incoming)
        for jp in range(pairs):
            start_run, start_h = starts[jp]
            carry = start_h + start_run * halves(turned[2 * jp:2 * jp + 1], incoming[2 * jp + 1:2 * jp + 2])
            out_gain = PAR[l, q, jp][5:6]
            for k in range(steps):
                rows = pl.ds(k, ROWS, stride=steps)
                MIX[jp, rows, :] = (LOC[jp, k] + ACU[jp, k] * carry) * GEL[jp, rows, :] * out_gain
            MX[l, q, :, jp * LANE:(jp + 1) * LANE] = MIX[jp].astype(bf16)
        return [put(MX.at[l, q], MX.at[l, q], s, tp_of(c, p, (q + d) % n)) for d in near]

    def update(l, emit):
        squares = jnp.zeros((tq, LANE), f32)
        for qq in range(n):
            for jp in range(pairs):
                v = MX[l, qq, :, jp * LANE:(jp + 1) * LANE].astype(f32) / PAR[l, qq, jp][5:6]
                squares = squares + v * v
        scale = lax.rsqrt(jnp.sum(squares, axis=1, keepdims=True) * (1.0 / (n * C)) + EPS)
        mixed = jnp.concatenate([MX[l, qq] for qq in range(n)], axis=1)
        for jp in range(pairs):
            w = jnp.concatenate(
                [WO[l, 2 * jp].reshape(n * C, LANE), WO[l, 2 * jp + 1].reshape(n * C, LANE)], axis=1)
            up = jnp.dot(mixed, w, preferred_element_type=f32) * scale
            for j in (0, 1):
                at = tp_of(c, 2 * jp + j, q)
                emit(2 * jp + j, (XM[l, at].astype(f32) + up[:, j * LANE:(j + 1) * LANE]).astype(bf16))

    landed(t_b)

    @pl.when(p > 0)
    def _():
        landed_all(XH.at[0, :nt - 1], rim0)

    @pl.when(p == 0)
    def _():
        landed_all(XH.at[0], rim0)

    norm(0)
    landed(wx[0])
    wx[0] = twin_x(0)
    landed(wout[0])
    wout[0] = twin_o(0)
    landed(wx[0])
    wx[0] = across(WX.at[0, p])
    landed(wout[0])
    wout[0] = across(WO.at[0, p])
    landed(wx[1])
    wx[1] = z2_x(1)
    landed(wout[1])
    wout[1] = z2_o(1)
    landed(wx[0])
    start = first_half(0)
    landed(wx[1])
    wx[1] = twin_x(1)
    landed(wout[1])
    wout[1] = twin_o(1)
    incoming = prefix(0)
    gathered = second_half(0, start, incoming)
    landed(wx[1])
    wx[1] = across(WX.at[1, p])
    landed(wout[1])
    wout[1] = across(WO.at[1, p])
    landed(wout[0])
    landed(gathered)

    def keep_stream(j, v):
        XM[1, tp_of(c, j, q)] = v

    update(0, keep_stream)
    gathered = []
    for d in near:
        for j in range(n):
            ref = XM.at[1, tp_of(c, j, q)]
            gathered.append(put(ref, ref, s, tp_of(c, p, (q + d) % n)))
    rim1 = next(numbers)
    e, pp = (p + 1) // n, (p + 1) % n
    for j in range(n):
        at = tp_of(c, j, q)
        for qq in range(n):
            put(XM.at[1, at, tq - RIM:tq], XH.at[1, at], (s + e) % ns, tp_of((c + e) % 2, pp, qq), rim1)
    landed(gathered)
    landed_all(XH.at[1], rim1)
    norm(1)
    landed(wx[1])
    start = first_half(1)
    incoming = prefix(1)
    gathered = second_half(1, start, incoming)
    landed(wout[1])
    landed(gathered)

    def keep_last(j, v):
        FS[j] = v

    update(1, keep_last)
    last = [put(FS.at[(p + d) % n], OB.at[p], s, tp_of(c, (p + d) % n, q)) for d in near]
    OB[p] = FS[p]
    landed(last)
    for k in range(n):
        out[k * tq:(k + 1) * tq] = OB[k]
    for cp in sent:
        cp.wait_send()
    for cp, mine in rim_sends:
        @pl.when(mine == 0)
        def _():
            cp.wait_send()


def body(tokens, mix_gain, x_weight, gate_weight, conv_taps, a_maps, i_maps, decay_rate, pace, jumps,
         out_gain, out_weight):
    nt = lax.axis_size("tp")
    n = int(round(nt ** 0.5))
    tq = tokens.shape[0] // n
    C = n * HEAD
    D = nt * LANE
    wxg = jnp.concatenate([x_weight, gate_weight], axis=2)
    maps = jnp.concatenate([a_maps[:, 0], i_maps[:, 0]], axis=2)
    small = jnp.concatenate(
        [conv_taps.astype(f32), decay_rate[:, None], out_gain.astype(f32)[:, None],
         jnp.ones((LAYERS, 2, HEAD), f32)], axis=1)
    small = jnp.concatenate([small, small], axis=2)
    pj = jnp.stack([pace, jumps], axis=1)
    vmem = pl.BlockSpec(memory_space=pltpu.VMEM)
    xr, orr = wxg.shape[1], out_weight.shape[1]
    scratch = [
        pltpu.VMEM((LAYERS, n, n, n, 2, xr, LANE), bf16),
        pltpu.VMEM((LAYERS, n, n, n, 2, orr, LANE), bf16),
        pltpu.VMEM((n, LAYERS, HEAD, LANE), bf16),
        pltpu.VMEM((nt, LAYERS, ROWS, LANE), f32),
        pltpu.VMEM((LAYERS, nt, tq, LANE), bf16),
        pltpu.VMEM((LAYERS, nt, RIM, LANE), bf16),
        pltpu.VMEM((RIM + tq, D), bf16),
        pltpu.VMEM((n // 2, RIM + tq, LANE), f32),
        pltpu.VMEM((n // 2, tq, LANE), f32),
        pltpu.VMEM((LAYERS, n // 2, LANE, 2 * LANE), bf16),
        pltpu.VMEM((LAYERS, n, n // 2, ROWS, LANE), f32),
        pltpu.VMEM((n // 2, tq, LANE), f32),
        pltpu.VMEM((n // 2, tq, LANE), f32),
        pltpu.VMEM((n // 2, tq // ROWS, ROWS, LANE), f32),
        pltpu.VMEM((n // 2, tq // ROWS, ROWS, LANE), f32),
        pltpu.VMEM((n // 2, tq, LANE), f32),
        pltpu.VMEM((LAYERS, n, tq, C), bf16),
        pltpu.VMEM((LAYERS, n, 1, LANE), f32),
        pltpu.VMEM((LAYERS, 2, n, n, 1, LANE), f32),
        pltpu.VMEM((LAYERS, n, 1, LANE), f32),
        pltpu.VMEM((LAYERS, nt - 1, n, 1, LANE), f32),
        pltpu.VMEM((n, tq, LANE), bf16),
        pltpu.VMEM((n, tq, LANE), bf16),
        pltpu.SemaphoreType.DMA,
        pltpu.SemaphoreType.DMA((256,)),
    ]
    return pl.pallas_call(
        functools.partial(kernel, n, tq),
        out_shape=jax.ShapeDtypeStruct(tokens.shape, bf16),
        in_specs=[vmem] * 7,
        out_specs=vmem,
        scratch_shapes=scratch,
        compiler_params=pltpu.CompilerParams(has_side_effects=True, vmem_limit_bytes=56 * 1024 * 1024),
    )(tokens, mix_gain, wxg, out_weight, maps, small, pj)


def solution(mesh):
    in_specs = (
        P("sp", "tp"),
        P(),
        P(None, "sp", "tp"),
        P(None, "sp", "tp"),
        P(None, None, "tp"),
        P(None, "tp", None, None),
        P(None, "tp", None, None),
        P(None, "tp"),
        P("sp"),
        P("sp"),
        P(None, "tp"),
        P(None, "sp", "tp"),
    )
    return jax.shard_map(body, mesh=mesh, in_specs=in_specs, out_specs=P("sp", "tp"), check_vma=False)
```

```python
import functools

import jax
import jax.numpy as jnp
from jax import lax
from jax.experimental import pallas as pl
from jax.experimental.pallas import tpu as pltpu
from jax.sharding import PartitionSpec as P

HEAD = 64
WIDTH = 4
LAYERS = 2
EPS = 1e-06
GATE_C = 8.0
RIM = 16
LANE = 128
ROWS = 8

f32 = jnp.float32
bf16 = jnp.bfloat16


def swapped(x):
    return pltpu.roll(x, HEAD, 1)


def lower_half(shape):
    return lax.broadcasted_iota(jnp.int32, shape, len(shape) - 1) < HEAD


def halves(first, second):
    return jnp.where(lower_half(first.shape), first, second)


def chained(first, second):
    low = lower_half(second.shape)
    return jnp.where(low, second, swapped(second)) * first + jnp.where(low, 0.0, second)


def gelu(x):
    return 0.5 * x * (1.0 + jnp.tanh(0.7978845608028654 * (x + 0.044715 * (x * x * x))))


def one_minus_exp(y, decay):
    series = jnp.ones_like(y)
    for k in range(8, 1, -1):
        series = 1.0 - (y * (1.0 / k)) * series
    return jnp.where(y < 0.5, y * series, 1.0 - decay * decay)


def kernel(n, tq, tok, gain, xw, gw, wo, taps, am, im, rate, og, pace, jumps, out,
           WXG, MAPO, SMO, PJ, WX, WO, MAPS, SMALL, XM, XH, NRM, XR, GEL, BD, PAR, AS, BS, LOC, ACU, MIX, MX,
           PO, PR, ZO, ZR, FS, OB, send, recv):
    nt, nz, ns = n * n, n * n, 2 * n * n
    C = n * HEAD
    pairs = n // 2
    D = nt * LANE
    steps = tq // ROWS
    s, tp = lax.axis_index("sp"), lax.axis_index("tp")
    c, z = s % 2, s // 2
    a, b = z // n, z % n
    y, x = tp // n, tp % n
    p, q = x + c * (y - x), y + c * (x - y)

    def tp_of(core, pp, qq):
        return (qq * n + pp) + core * ((pp * n + qq) - (qq * n + pp))

    sent = []
    numbers = iter(range(10000))

    def put(src, dst, sp_to, tp_to, slot=None):
        slot = next(numbers) if slot is None else slot
        cp = pltpu.make_async_remote_copy(
            src_ref=src, dst_ref=dst, send_sem=send, recv_sem=recv.at[slot],
            device_id={"sp": sp_to, "tp": tp_to}, device_id_type=pl.DeviceIdType.MESH)
        cp.start()
        sent.append(cp)
        return cp

    def landed(copies):
        for cp in copies:
            cp.wait_recv()

    def landed_all(ref, slot):
        pltpu.make_async_copy(ref, ref, recv.at[slot]).wait()

    near = range(1, n)
    half = n * n // 4
    across = 1 - c

    barrier = pltpu.get_barrier_semaphore()

    def greet(sp_to, tp_to):
        pl.semaphore_signal(barrier, inc=1, device_id={"sp": sp_to, "tp": tp_to},
                            device_id_type=pl.DeviceIdType.MESH)

    def zat(d, core=None):
        return ((z + d + nz) % nz) * 2 + (c if core is None else core)

    zs = sorted({d % nz for d in (1, 2, -1, -2)})
    for d in near:
        greet(s, tp_of(c, (p + d) % n, q))
        greet(s, tp_of(c, p, (q + d) % n))
    for d in range(n):
        greet(z * 2 + across, tp_of(across, q, d))
    for d in zs:
        greet(zat(d), tp)

    @pl.when((1 - c) * (1 - jnp.minimum(p, 1)) == 1)
    def _():
        for k in range(n):
            greet(zat(-1, 1), tp_of(1, q, k))

    for l in range(LAYERS):
        WXG[l] = jnp.concatenate([xw[l], gw[l]], axis=1)
        MAPO[l] = jnp.concatenate([am[l, 0], im[l, 0]], axis=1)
        rows = jnp.concatenate(
            [taps[l].astype(f32), rate[l:l + 1], og[l:l + 1].astype(f32), jnp.ones((2, HEAD), f32)], axis=0)
        SMO[l] = jnp.concatenate([rows, rows], axis=1)
    for i, ref in enumerate((pace, jumps)):
        for r in range(n * tq // LANE):
            PJ[i, r * LANE:(r + 1) * LANE] = jnp.transpose(jnp.broadcast_to(ref[r:r + 1], (LANE, LANE)))
    pl.semaphore_wait(barrier, 2 * (n - 1) + n + len(zs) + c)

    def x_piece(l, o):
        return WX.at[l, p, o, c]

    def o_piece(l, o):
        i, k = o // n, o % n
        return WO.at[l, p, i + c * (k - i), k + c * (i - k), c]

    def ring_numbers():
        first = next(numbers)
        for _ in range(4 * half - 1):
            next(numbers)
        return first

    def ring_send(piece, own, l, k, first):
        for sign, i in ((1, 0), (-1, 2)):
            o = (z - sign * 2 * k + nz) % nz
            dst = piece(l, o)
            src = own if k == 0 else dst
            put(src, dst, zat(sign), tp, first + 4 * k + i)
            if sign == 1 or k < half - 1:
                put(src, dst, zat(2 * sign), tp, first + 4 * k + i + 1)

    def ring_land(piece, l, k, first):
        got = []
        for sign, i in ((1, 0), (-1, 2)):
            for j in (1, 2):
                if j == 2 and sign == -1 and k == half - 1:
                    continue
                o = (z - sign * (2 * k + j) + nz) % nz
                landed_all(piece(l, o), first + 4 * k + i + j - 1)
                got.append(o)
        return got

    same, other = next(numbers), next(numbers)

    def spread(o, src=None):
        ref = WX.at[0, p, o, c]
        src = ref if src is None else src
        for d in near:
            put(src, ref, s, tp_of(c, (p + d) % n, q), same)
        for d in range(n):
            put(src, WX.at[0, q, o, c], z * 2 + across, tp_of(across, (q + d) % n, p), other)

    def spread_x(l):
        made = [put(WX.at[l, p, :, c], WX.at[l, p, :, c], s, tp_of(c, (p + d) % n, q)) for d in near]
        for d in range(n):
            made.append(put(WX.at[l, p, :, c], WX.at[l, q, :, c], z * 2 + across, tp_of(across, (q + d) % n, p)))
        return made

    def spread_o(l):
        made = [put(WO.at[l, p, :, :, c], WO.at[l, p, :, :, c], s, tp_of(c, (p + d) % n, q)) for d in near]
        for d in range(n):
            for k in range(n):
                made.append(put(WO.at[l, p, k, :, c], WO.at[l, q, :, k, c], z * 2 + across,
                                tp_of(across, (q + d) % n, p)))
        return made

    firsts = {(kind, l): ring_numbers() for l in range(LAYERS) for kind in "xo"}

    own = pl.ds(pl.multiple_of(p * tq, tq), tq)
    t_a = []
    for d in near:
        pp = (p + d) % n
        rows = pl.ds(pl.multiple_of(pp * tq, tq), tq)
        t_a.append(put(tok.at[rows], XM.at[0, tp], s, tp_of(c, pp, q)))
    rim0 = next(numbers)
    rim_sends = []
    for k in range(n - 1):
        src = tok.at[(k + 1) * tq - RIM:(k + 1) * tq]
        cp = pltpu.make_async_remote_copy(
            src_ref=src, dst_ref=XH.at[0, tp], send_sem=send, recv_sem=recv.at[rim0],
            device_id={"sp": s, "tp": tp_of(c, k + 1, q)}, device_id_type=pl.DeviceIdType.MESH)

        @pl.when(p != k + 1)
        def _():
            cp.start()

        @pl.when(p == k + 1)
        def _():
            XH[0, tp] = src[...]
        rim_sends.append((cp, k + 1))
    put(tok.at[n * tq - RIM:n * tq], XH.at[0, tp], (s + 1) % ns, tp_of(across, 0, p), rim0)
    ring_send(x_piece, WXG.at[0], 0, 0, firsts["x", 0])
    spread(z, WXG.at[0])
    m_in = [put(MAPO, MAPS.at[p], s, tp_of(c, (p + d) % n, q)) for d in near]
    s_in = [put(SMO, SMALL.at[p], s, tp_of(c, (p + d) % n, q)) for d in near]
    ring_send(o_piece, wo.at[0], 0, 0, firsts["o", 0])

    XM[0, tp] = tok[own]
    for l in range(LAYERS):
        WX[l, p, z, c] = WXG[l]
        WO[l, p, a + c * (b - a), b + c * (a - b), c] = wo[l]
    MAPS[p] = MAPO[...]
    SMALL[p] = SMO[...]

    landed(t_a)

    @pl.when(p > 0)
    def _():
        landed_all(XH.at[0, :n - 1], rim0)

    @pl.when(p == 0)
    def _():
        landed_all(XH.at[0, :n], rim0)

    t_b = []
    for d in near:
        to = tp_of(c, p, (q + d) % n)
        t_b.append(put(tok.at[own], XM.at[0, tp], s, to))
        for e in near:
            ref = XM.at[0, tp_of(c, (p + e) % n, q)]
            t_b.append(put(ref, ref, s, to))
        for e in range(n):
            ref = XH.at[0, tp_of(c, (p + e) % n, q)]
            t_b.append(put(ref, ref, s, to))

    def ring_step(k):
        if k < half:
            got = ring_land(x_piece, 0, k - 1, firsts["x", 0])
            ring_send(x_piece, None, 0, k, firsts["x", 0])
        else:
            got = ring_land(x_piece, 0, half - 1, firsts["x", 0])
        for o in got:
            spread(o)
        ring_land(o_piece, 0, k - 1, firsts["o", 0])
        if k < half:
            ring_send(o_piece, None, 0, k, firsts["o", 0])

    def ring_step1(k):
        for kind, piece, mine in (("x", x_piece, WXG), ("o", o_piece, wo)):
            if k > 0:
                ring_land(piece, 1, k - 1, firsts[kind, 1])
            if k < half:
                ring_send(piece, mine.at[1], 1, k, firsts[kind, 1])

    for k in range(1, half):
        ring_step(k)
        ring_step1(k - 1)

    landed(m_in)
    landed(s_in)
    for l in range(LAYERS):
        for jp in range(pairs):
            even = MAPS[2 * jp, l].astype(f32)
            odd = MAPS[2 * jp + 1, l].astype(f32)
            low = lower_half(even.shape)
            BD[l, jp, :HEAD, :LANE] = jnp.where(low, even, 0.0).astype(bf16)
            BD[l, jp, :HEAD, LANE:] = jnp.where(low, swapped(even), 0.0).astype(bf16)
            BD[l, jp, HEAD:, :LANE] = jnp.where(low, 0.0, swapped(odd)).astype(bf16)
            BD[l, jp, HEAD:, LANE:] = jnp.where(low, 0.0, odd).astype(bf16)
            PAR[l, q, jp] = halves(SMALL[2 * jp, l], SMALL[2 * jp + 1, l])

    def norm_rows(l, block, row):
        total = jnp.zeros((RIM, LANE), f32)
        for t in range(nt):
            v = block(t).astype(f32)
            total = total + v * v
        r = lax.rsqrt(jnp.sum(total, axis=1, keepdims=True) * (1.0 / D) + EPS)
        for t in range(nt):
            cols = slice(t * LANE, (t + 1) * LANE)
            g = gain[l:l + 1, cols].astype(f32)
            NRM[pl.ds(row, RIM), cols] = (block(t).astype(f32) * r * g).astype(bf16)

    def norm(l):
        norm_rows(l, lambda t: XH[l, t], 0)

        @pl.loop(0, tq // RIM)
        def _(i):
            row = pl.multiple_of(i * RIM, RIM)
            norm_rows(l, lambda t: XM[l, t, pl.ds(row, RIM), :], pl.multiple_of(row + RIM, RIM))

    def first_half(l):
        keep = jnp.minimum(s + p, 1).astype(f32)
        normed = NRM[...]
        speed = PJ[0, own, :]
        jump = PJ[1, own, :]
        for jp in range(pairs):
            w = jnp.concatenate(
                [WX[l, 2 * jp].reshape(D, LANE), WX[l, 2 * jp + 1].reshape(D, LANE)], axis=1)
            pr = jnp.dot(normed, w, preferred_element_type=f32).astype(bf16).astype(f32)
            left, right = pr[:, :LANE], pr[:, LANE:]
            xr = halves(left, swapped(right))
            XR[jp, :RIM] = xr[:RIM] * keep
            XR[jp, RIM:] = xr[RIM:]
            GEL[jp] = gelu(halves(swapped(left), right)[RIM:])
            par = PAR[l, q, jp]
            conv = jnp.zeros((tq, LANE), f32)
            for k in range(WIDTH):
                conv = conv + par[k:k + 1] * XR[jp, pl.ds(RIM - WIDTH + 1 + k, tq), :]
            xc = conv.astype(bf16)
            gates = jnp.dot(xc, BD[l, jp], preferred_element_type=f32)
            r = jax.nn.sigmoid(gates[:, :LANE])
            gin = jax.nn.sigmoid(gates[:, LANE:])
            log_a = -GATE_C * r * par[4:5] * speed + jump
            decay = jnp.exp(log_a)
            AS[jp] = decay
            BS[jp] = jnp.sqrt(one_minus_exp(-2.0 * log_a, decay)) * gin * xc.astype(f32)
        starts = []
        for jp in range(pairs):
            run = h = None
            for k in range(steps):
                ak = AS[jp, pl.ds(k, ROWS, stride=steps), :]
                bk = BS[jp, pl.ds(k, ROWS, stride=steps), :]
                h = bk if k == 0 else ak * h + bk
                run = ak if k == 0 else ak * run
                LOC[jp, k], ACU[jp, k] = h, run
            row = lax.broadcasted_iota(jnp.int32, (ROWS, LANE), 0)
            for d in (1, 2, 4):
                before = row >= d
                h = run * jnp.where(before, pltpu.roll(h, d, 0), 0.0) + h
                run = run * jnp.where(before, pltpu.roll(run, d, 0), 1.0)
            av, sv = run[ROWS - 1:], h[ROWS - 1:]
            PO[l, 2 * jp] = halves(av, swapped(sv))
            PO[l, 2 * jp + 1] = halves(swapped(av), sv)
            starts.append((jnp.where(row >= 1, pltpu.roll(run, 1, 0), 1.0),
                           jnp.where(row >= 1, pltpu.roll(h, 1, 0), 0.0)))
        return starts

    def prefix(l):
        made = []
        for d in near:
            made.append(put(PO.at[l], PR.at[l, c, p], s, tp_of(c, (p + d) % n, q)))
        slot = next(numbers)
        for k in range(n):
            for pp in range(n):
                put(PO.at[l, k], PR.at[l, c, p, q], z * 2 + 1 - c, tp_of(1 - c, pp, k), slot)
        for j in range(n):
            PR[l, c, p, j] = PO[l, j]
        landed(made)
        landed_all(PR.at[l, 1 - c], slot)
        identity = jnp.where(lower_half((n, LANE)), 1.0, 0.0)
        total = within = identity
        mine = c * n + p
        for i in range(2 * n):
            piece = jnp.concatenate([PR[l, i // n, i % n, j] for j in range(n)], axis=0)
            within = jnp.where(i < mine, chained(within, piece), within)
            total = chained(total, piece)
        for j in range(n):
            ZO[l, j] = total[j:j + 1]
        slot = next(numbers)
        for d in range(1, nz):
            put(ZO.at[l], ZR.at[l, d - 1], ((z + d) % nz) * 2 + c, tp, slot)
        landed_all(ZR.at[l], slot)
        before = identity
        for d in range(nz - 1, 0, -1):
            piece = jnp.concatenate([ZR[l, d - 1, j] for j in range(n)], axis=0)
            before = jnp.where(d <= z, chained(before, piece), before)
        return chained(before, within)

    def second_half(l, starts, incoming):
        turned = swapped(incoming)
        for jp in range(pairs):
            start_run, start_h = starts[jp]
            carry = start_h + start_run * halves(turned[2 * jp:2 * jp + 1], incoming[2 * jp + 1:2 * jp + 2])
            out_gain = PAR[l, q, jp][5:6]
            for k in range(steps):
                rows = pl.ds(k, ROWS, stride=steps)
                MIX[jp, rows, :] = (LOC[jp, k] + ACU[jp, k] * carry) * GEL[jp, rows, :] * out_gain
            MX[l, q, :, jp * LANE:(jp + 1) * LANE] = MIX[jp].astype(bf16)
        return [put(MX.at[l, q], MX.at[l, q], s, tp_of(c, p, (q + d) % n)) for d in near]

    def update(l, emit):
        squares = jnp.zeros((tq, LANE), f32)
        for qq in range(n):
            for jp in range(pairs):
                v = MX[l, qq, :, jp * LANE:(jp + 1) * LANE].astype(f32) / PAR[l, qq, jp][5:6]
                squares = squares + v * v
        scale = lax.rsqrt(jnp.sum(squares, axis=1, keepdims=True) * (1.0 / (n * C)) + EPS)
        mixed = jnp.concatenate([MX[l, qq] for qq in range(n)], axis=1)
        for jp in range(pairs):
            w = jnp.concatenate(
                [WO[l, 2 * jp].reshape(n * C, LANE), WO[l, 2 * jp + 1].reshape(n * C, LANE)], axis=1)
            up = jnp.dot(mixed, w, preferred_element_type=f32) * scale
            for j in (0, 1):
                at = tp_of(c, 2 * jp + j, q)
                emit(2 * jp + j, (XM[l, at].astype(f32) + up[:, j * LANE:(j + 1) * LANE]).astype(bf16))

    par_in = [put(PAR.at[:, q], PAR.at[:, q], s, tp_of(c, p, (q + d) % n)) for d in near]
    landed(t_b)
    ring_step(half)
    ring_step1(half - 1)
    o_in = [spread_o(0), None]
    norm(0)
    ring_step1(half)
    x_in = spread_x(1)
    landed_all(WX.at[0, 0:n - 1, :, 0], same)
    landed_all(WX.at[0, :, :, 0], other)
    start = first_half(0)
    incoming = prefix(0)
    gathered = second_half(0, start, incoming)
    landed(par_in)
    landed(o_in[0])
    landed(gathered)

    def keep_stream(j, v):
        XM[1, tp_of(c, j, q)] = v

    update(0, keep_stream)
    gathered = []
    for d in near:
        for j in range(n):
            ref = XM.at[1, tp_of(c, j, q)]
            gathered.append(put(ref, ref, s, tp_of(c, p, (q + d) % n)))
    rim1 = next(numbers)
    e, pp = (p + 1) // n, (p + 1) % n
    for j in range(n):
        at = tp_of(c, j, q)
        for qq in range(n):
            put(XM.at[1, at, tq - RIM:tq], XH.at[1, at], (s + e) % ns, tp_of((c + e) % 2, pp, qq), rim1)
    landed(gathered)
    landed_all(XH.at[1], rim1)
    norm(1)
    landed(x_in)
    start = first_half(1)
    o_in[1] = spread_o(1)
    incoming = prefix(1)
    gathered = second_half(1, start, incoming)
    landed(o_in[1])
    landed(gathered)

    def keep_last(j, v):
        FS[j] = v

    update(1, keep_last)
    last = [put(FS.at[(p + d) % n], OB.at[p], s, tp_of(c, (p + d) % n, q)) for d in near]
    OB[p] = FS[p]
    landed(last)
    for k in range(n):
        out[k * tq:(k + 1) * tq] = OB[k]
    for cp in sent:
        cp.wait_send()
    for cp, k in rim_sends:
        @pl.when(p != k)
        def _():
            cp.wait_send()


def body(tokens, mix_gain, x_weight, gate_weight, conv_taps, a_maps, i_maps, decay_rate, pace, jumps,
         out_gain, out_weight):
    nt = lax.axis_size("tp")
    n = int(round(nt ** 0.5))
    tq = tokens.shape[0] // n
    C = n * HEAD
    D = nt * LANE
    lines = (-1, LANE)
    vmem = pl.BlockSpec(memory_space=pltpu.VMEM)
    xr, orr = x_weight.shape[1], out_weight.shape[1]
    scratch = [
        pltpu.VMEM((LAYERS, xr, LANE), bf16),
        pltpu.VMEM((LAYERS, HEAD, LANE), bf16),
        pltpu.VMEM((LAYERS, ROWS, LANE), f32),
        pltpu.VMEM((2, n * tq, LANE), f32),
        pltpu.VMEM((LAYERS, n, nt, 2, xr, LANE), bf16),
        pltpu.VMEM((LAYERS, n, n, n, 2, orr, LANE), bf16),
        pltpu.VMEM((n, LAYERS, HEAD, LANE), bf16),
        pltpu.VMEM((n, LAYERS, ROWS, LANE), f32),
        pltpu.VMEM((LAYERS, nt, tq, LANE), bf16),
        pltpu.VMEM((LAYERS, nt, RIM, LANE), bf16),
        pltpu.VMEM((RIM + tq, D), bf16),
        pltpu.VMEM((n // 2, RIM + tq, LANE), f32),
        pltpu.VMEM((n // 2, tq, LANE), f32),
        pltpu.VMEM((LAYERS, n // 2, LANE, 2 * LANE), bf16),
        pltpu.VMEM((LAYERS, n, n // 2, ROWS, LANE), f32),
        pltpu.VMEM((n // 2, tq, LANE), f32),
        pltpu.VMEM((n // 2, tq, LANE), f32),
        pltpu.VMEM((n // 2, tq // ROWS, ROWS, LANE), f32),
        pltpu.VMEM((n // 2, tq // ROWS, ROWS, LANE), f32),
        pltpu.VMEM((n // 2, tq, LANE), f32),
        pltpu.VMEM((LAYERS, n, tq, C), bf16),
        pltpu.VMEM((LAYERS, n, 1, LANE), f32),
        pltpu.VMEM((LAYERS, 2, n, n, 1, LANE), f32),
        pltpu.VMEM((LAYERS, n, 1, LANE), f32),
        pltpu.VMEM((LAYERS, nt - 1, n, 1, LANE), f32),
        pltpu.VMEM((n, tq, LANE), bf16),
        pltpu.VMEM((n, tq, LANE), bf16),
        pltpu.SemaphoreType.DMA,
        pltpu.SemaphoreType.DMA((320,)),
    ]
    return pl.pallas_call(
        functools.partial(kernel, n, tq),
        out_shape=jax.ShapeDtypeStruct(tokens.shape, bf16),
        in_specs=[vmem] * 12,
        out_specs=vmem,
        scratch_shapes=scratch,
        compiler_params=pltpu.CompilerParams(collective_id=0, has_side_effects=True, vmem_limit_bytes=56 * 1024 * 1024),
    )(tokens, mix_gain, x_weight, gate_weight, out_weight, conv_taps, a_maps, i_maps, decay_rate, out_gain,
      pace.reshape(lines), jumps.reshape(lines))


def solution(mesh):
    in_specs = (
        P("sp", "tp"),
        P(),
        P(None, "sp", "tp"),
        P(None, "sp", "tp"),
        P(None, None, "tp"),
        P(None, "tp", None, None),
        P(None, "tp", None, None),
        P(None, "tp"),
        P("sp"),
        P("sp"),
        P(None, "tp"),
        P(None, "sp", "tp"),
    )
    return jax.shard_map(body, mesh=mesh, in_specs=in_specs, out_specs=P("sp", "tp"), check_vma=False)
```

```python
import functools

import jax
import jax.numpy as jnp
from jax import lax
from jax.experimental import pallas as pl
from jax.experimental.pallas import tpu as pltpu
from jax.sharding import PartitionSpec as P

HEAD = 64
WIDTH = 4
LAYERS = 2
EPS = 1e-06
GATE_C = 8.0
RIM = 16
LANE = 128
ROWS = 8

f32 = jnp.float32
bf16 = jnp.bfloat16


def swapped(x):
    return pltpu.roll(x, HEAD, 1)


def lower_half(shape):
    return lax.broadcasted_iota(jnp.int32, shape, len(shape) - 1) < HEAD


def halves(first, second):
    return jnp.where(lower_half(first.shape), first, second)


def chained(first, second):
    low = lower_half(second.shape)
    return jnp.where(low, second, swapped(second)) * first + jnp.where(low, 0.0, second)


def gelu(x):
    return 0.5 * x * (1.0 + jnp.tanh(0.7978845608028654 * (x + 0.044715 * (x * x * x))))


def one_minus_exp(y, decay):
    series = jnp.ones_like(y)
    for k in range(8, 1, -1):
        series = 1.0 - (y * (1.0 / k)) * series
    return jnp.where(y < 0.5, y * series, 1.0 - decay * decay)


def kernel(n, tq, tok, gain, xw, gw, wo, taps, am, im, rate, og, pace, jumps, out,
           WXG, MAPO, SMO, PJ, WX, WO, MAPS, SMALL, XM, XH, NRM, XR, GEL, BD, PAR, AS, BS, LOC, ACU, MIX, MX,
           PO, PR, ZO, ZR, FS, OB, send, recv):
    nt, nz, ns = n * n, n * n, 2 * n * n
    C = n * HEAD
    pairs = n // 2
    D = nt * LANE
    steps = tq // ROWS
    s, tp = lax.axis_index("sp"), lax.axis_index("tp")
    c, z = s % 2, s // 2
    a, b = z // n, z % n
    y, x = tp // n, tp % n
    p, q = x + c * (y - x), y + c * (x - y)

    def tp_of(core, pp, qq):
        return (qq * n + pp) + core * ((pp * n + qq) - (qq * n + pp))

    sent = []
    numbers = iter(range(10000))

    def put(src, dst, sp_to, tp_to, slot=None):
        slot = next(numbers) if slot is None else slot
        cp = pltpu.make_async_remote_copy(
            src_ref=src, dst_ref=dst, send_sem=send, recv_sem=recv.at[slot],
            device_id={"sp": sp_to, "tp": tp_to}, device_id_type=pl.DeviceIdType.MESH)
        cp.start()
        sent.append(cp)
        return cp

    def landed(copies):
        for cp in copies:
            cp.wait_recv()

    def landed_all(ref, slot):
        pltpu.make_async_copy(ref, ref, recv.at[slot]).wait()

    near = range(1, n)
    half = n * n // 4
    across = 1 - c

    barrier = pltpu.get_barrier_semaphore()

    def greet(sp_to, tp_to):
        pl.semaphore_signal(barrier, inc=1, device_id={"sp": sp_to, "tp": tp_to},
                            device_id_type=pl.DeviceIdType.MESH)

    def zat(d, core=None):
        return ((z + d + nz) % nz) * 2 + (c if core is None else core)

    zs = sorted({d % nz for d in (1, 2, -1, -2)})
    for d in near:
        greet(s, tp_of(c, (p + d) % n, q))
        greet(s, tp_of(c, p, (q + d) % n))
    for d in range(n):
        greet(z * 2 + across, tp_of(across, q, d))
    for d in zs:
        greet(zat(d), tp)

    @pl.when((1 - c) * (1 - jnp.minimum(p, 1)) == 1)
    def _():
        for k in range(n):
            greet(zat(-1, 1), tp_of(1, q, k))

    for l in range(LAYERS):
        WXG[l] = jnp.concatenate([xw[l], gw[l]], axis=1)
        MAPO[l] = jnp.concatenate([am[l, 0], im[l, 0]], axis=1)
        rows = jnp.concatenate(
            [taps[l].astype(f32), rate[l:l + 1], og[l:l + 1].astype(f32), jnp.ones((2, HEAD), f32)], axis=0)
        SMO[l] = jnp.concatenate([rows, rows], axis=1)
    for i, ref in enumerate((pace, jumps)):
        for r in range(n * tq // LANE):
            PJ[i, r * LANE:(r + 1) * LANE] = jnp.transpose(jnp.broadcast_to(ref[r:r + 1], (LANE, LANE)))
    pl.semaphore_wait(barrier, 2 * (n - 1) + n + len(zs) + c)

    def x_piece(l, o):
        return WX.at[l, p, o, c]

    def o_piece(l, o):
        i, k = o // n, o % n
        return WO.at[l, p, i + c * (k - i), k + c * (i - k), c]

    def ring_numbers():
        first = next(numbers)
        for _ in range(4 * half - 1):
            next(numbers)
        return first

    def ring_send(piece, own, l, k, first):
        for sign, i in ((1, 0), (-1, 2)):
            o = (z - sign * 2 * k + nz) % nz
            dst = piece(l, o)
            src = own if k == 0 else dst
            put(src, dst, zat(sign), tp, first + 4 * k + i)
            if sign == 1 or k < half - 1:
                put(src, dst, zat(2 * sign), tp, first + 4 * k + i + 1)

    def ring_land(piece, l, k, first):
        got = []
        for sign, i in ((1, 0), (-1, 2)):
            for j in (1, 2):
                if j == 2 and sign == -1 and k == half - 1:
                    continue
                o = (z - sign * (2 * k + j) + nz) % nz
                landed_all(piece(l, o), first + 4 * k + i + j - 1)
                got.append(o)
        return got

    same, other = next(numbers), next(numbers)

    def spread(o, src=None):
        ref = WX.at[0, p, o, c]
        src = ref if src is None else src
        for d in near:
            put(src, ref, s, tp_of(c, (p + d) % n, q), same)
        for d in range(n):
            put(src, WX.at[0, q, o, c], z * 2 + across, tp_of(across, (q + d) % n, p), other)

    def spread_x(l, first, last):
        part = pl.ds(first, last - first)
        made = [put(WX.at[l, p, part, c], WX.at[l, p, part, c], s, tp_of(c, (p + d) % n, q)) for d in near]
        for d in range(n):
            made.append(put(WX.at[l, p, part, c], WX.at[l, q, part, c], z * 2 + across,
                            tp_of(across, (q + d) % n, p)))
        return made

    def far_first(l):
        made = []
        for d in near:
            to = (((a + d) % n) * n + b) * 2 + c
            made.append(put(WXG.at[l], x_piece(l, z), to, tp))
            made.append(put(wo.at[l], o_piece(l, z), to, tp))
        return made

    def near_next(l):
        made = []
        for piece in (x_piece, o_piece):
            for d in near:
                for k in range(n):
                    ref = piece(l, k * n + b)
                    made.append(put(ref, ref, (a * n + (b + d) % n) * 2 + c, tp))
        return made

    def spread_o(l):
        made = [put(WO.at[l, p, :, :, c], WO.at[l, p, :, :, c], s, tp_of(c, (p + d) % n, q)) for d in near]
        for d in range(n):
            for k in range(n):
                made.append(put(WO.at[l, p, k, :, c], WO.at[l, q, :, k, c], z * 2 + across,
                                tp_of(across, (q + d) % n, p)))
        return made

    firsts = {(kind, 0): ring_numbers() for kind in "xo"}

    own = pl.ds(pl.multiple_of(p * tq, tq), tq)
    t_a = []
    for d in near:
        pp = (p + d) % n
        rows = pl.ds(pl.multiple_of(pp * tq, tq), tq)
        t_a.append(put(tok.at[rows], XM.at[0, tp], s, tp_of(c, pp, q)))
    rim0 = next(numbers)
    rim_sends = []
    for k in range(n - 1):
        src = tok.at[(k + 1) * tq - RIM:(k + 1) * tq]
        cp = pltpu.make_async_remote_copy(
            src_ref=src, dst_ref=XH.at[0, tp], send_sem=send, recv_sem=recv.at[rim0],
            device_id={"sp": s, "tp": tp_of(c, k + 1, q)}, device_id_type=pl.DeviceIdType.MESH)

        @pl.when(p != k + 1)
        def _():
            cp.start()

        @pl.when(p == k + 1)
        def _():
            XH[0, tp] = src[...]
        rim_sends.append((cp, k + 1))
    put(tok.at[n * tq - RIM:n * tq], XH.at[0, tp], (s + 1) % ns, tp_of(across, 0, p), rim0)
    ring_send(x_piece, WXG.at[0], 0, 0, firsts["x", 0])
    spread(z, WXG.at[0])
    m_in = [put(MAPO, MAPS.at[p], s, tp_of(c, (p + d) % n, q)) for d in near]
    s_in = [put(SMO, SMALL.at[p], s, tp_of(c, (p + d) % n, q)) for d in near]
    ring_send(o_piece, wo.at[0], 0, 0, firsts["o", 0])

    XM[0, tp] = tok[own]
    for l in range(LAYERS):
        WX[l, p, z, c] = WXG[l]
        WO[l, p, a + c * (b - a), b + c * (a - b), c] = wo[l]
    MAPS[p] = MAPO[...]
    SMALL[p] = SMO[...]

    landed(t_a)

    @pl.when(p > 0)
    def _():
        landed_all(XH.at[0, :n - 1], rim0)

    @pl.when(p == 0)
    def _():
        landed_all(XH.at[0, :n], rim0)

    t_b = []
    for d in near:
        to = tp_of(c, p, (q + d) % n)
        t_b.append(put(tok.at[own], XM.at[0, tp], s, to))
        for e in near:
            ref = XM.at[0, tp_of(c, (p + e) % n, q)]
            t_b.append(put(ref, ref, s, to))
        for e in range(n):
            ref = XH.at[0, tp_of(c, (p + e) % n, q)]
            t_b.append(put(ref, ref, s, to))

    def ring_step(k):
        if k < half:
            got = ring_land(x_piece, 0, k - 1, firsts["x", 0])
            ring_send(x_piece, None, 0, k, firsts["x", 0])
        else:
            got = ring_land(x_piece, 0, half - 1, firsts["x", 0])
        for o in got:
            spread(o)
        ring_land(o_piece, 0, k - 1, firsts["o", 0])
        if k < half:
            ring_send(o_piece, None, 0, k, firsts["o", 0])

    for k in range(1, half):
        ring_step(k)

    landed(m_in)
    landed(s_in)
    for l in range(LAYERS):
        for jp in range(pairs):
            even = MAPS[2 * jp, l].astype(f32)
            odd = MAPS[2 * jp + 1, l].astype(f32)
            low = lower_half(even.shape)
            BD[l, jp, :HEAD, :LANE] = jnp.where(low, even, 0.0).astype(bf16)
            BD[l, jp, :HEAD, LANE:] = jnp.where(low, swapped(even), 0.0).astype(bf16)
            BD[l, jp, HEAD:, :LANE] = jnp.where(low, 0.0, swapped(odd)).astype(bf16)
            BD[l, jp, HEAD:, LANE:] = jnp.where(low, 0.0, odd).astype(bf16)
            PAR[l, q, jp] = halves(SMALL[2 * jp, l], SMALL[2 * jp + 1, l])

    def norm_rows(l, block, row):
        total = jnp.zeros((RIM, LANE), f32)
        for t in range(nt):
            v = block(t).astype(f32)
            total = total + v * v
        r = lax.rsqrt(jnp.sum(total, axis=1, keepdims=True) * (1.0 / D) + EPS)
        for t in range(nt):
            cols = slice(t * LANE, (t + 1) * LANE)
            g = gain[l:l + 1, cols].astype(f32)
            NRM[pl.ds(row, RIM), cols] = (block(t).astype(f32) * r * g).astype(bf16)

    def norm(l):
        norm_rows(l, lambda t: XH[l, t], 0)

        @pl.loop(0, tq // RIM)
        def _(i):
            row = pl.multiple_of(i * RIM, RIM)
            norm_rows(l, lambda t: XM[l, t, pl.ds(row, RIM), :], pl.multiple_of(row + RIM, RIM))

    def first_half(l):
        keep = jnp.minimum(s + p, 1).astype(f32)
        normed = NRM[...]
        speed = PJ[0, own, :]
        jump = PJ[1, own, :]
        for jp in range(pairs):
            w = jnp.concatenate(
                [WX[l, 2 * jp].reshape(D, LANE), WX[l, 2 * jp + 1].reshape(D, LANE)], axis=1)
            pr = jnp.dot(normed, w, preferred_element_type=f32).astype(bf16).astype(f32)
            left, right = pr[:, :LANE], pr[:, LANE:]
            xr = halves(left, swapped(right))
            XR[jp, :RIM] = xr[:RIM] * keep
            XR[jp, RIM:] = xr[RIM:]
            GEL[jp] = gelu(halves(swapped(left), right)[RIM:])
            par = PAR[l, q, jp]
            conv = jnp.zeros((tq, LANE), f32)
            for k in range(WIDTH):
                conv = conv + par[k:k + 1] * XR[jp, pl.ds(RIM - WIDTH + 1 + k, tq), :]
            xc = conv.astype(bf16)
            gates = jnp.dot(xc, BD[l, jp], preferred_element_type=f32)
            r = jax.nn.sigmoid(gates[:, :LANE])
            gin = jax.nn.sigmoid(gates[:, LANE:])
            log_a = -GATE_C * r * par[4:5] * speed + jump
            decay = jnp.exp(log_a)
            AS[jp] = decay
            BS[jp] = jnp.sqrt(one_minus_exp(-2.0 * log_a, decay)) * gin * xc.astype(f32)
        starts = []
        for jp in range(pairs):
            run = h = None
            for k in range(steps):
                ak = AS[jp, pl.ds(k, ROWS, stride=steps), :]
                bk = BS[jp, pl.ds(k, ROWS, stride=steps), :]
                h = bk if k == 0 else ak * h + bk
                run = ak if k == 0 else ak * run
                LOC[jp, k], ACU[jp, k] = h, run
            row = lax.broadcasted_iota(jnp.int32, (ROWS, LANE), 0)
            for d in (1, 2, 4):
                before = row >= d
                h = run * jnp.where(before, pltpu.roll(h, d, 0), 0.0) + h
                run = run * jnp.where(before, pltpu.roll(run, d, 0), 1.0)
            av, sv = run[ROWS - 1:], h[ROWS - 1:]
            PO[l, 2 * jp] = halves(av, swapped(sv))
            PO[l, 2 * jp + 1] = halves(swapped(av), sv)
            starts.append((jnp.where(row >= 1, pltpu.roll(run, 1, 0), 1.0),
                           jnp.where(row >= 1, pltpu.roll(h, 1, 0), 0.0)))
        return starts

    def prefix(l, meanwhile):
        made = []
        for d in near:
            made.append(put(PO.at[l], PR.at[l, c, p], s, tp_of(c, (p + d) % n, q)))
        slot = next(numbers)
        for k in range(n):
            for pp in range(n):
                put(PO.at[l, k], PR.at[l, c, p, q], z * 2 + 1 - c, tp_of(1 - c, pp, k), slot)
        for j in range(n):
            PR[l, c, p, j] = PO[l, j]
        landed(made)
        landed_all(PR.at[l, 1 - c], slot)
        identity = jnp.where(lower_half((n, LANE)), 1.0, 0.0)
        total = within = identity
        mine = c * n + p
        for i in range(2 * n):
            piece = jnp.concatenate([PR[l, i // n, i % n, j] for j in range(n)], axis=0)
            within = jnp.where(i < mine, chained(within, piece), within)
            total = chained(total, piece)
        for j in range(n):
            ZO[l, j] = total[j:j + 1]
        slot = next(numbers)
        for d in range(1, nz):
            put(ZO.at[l], ZR.at[l, d - 1], ((z + d) % nz) * 2 + c, tp, slot)
        meanwhile()
        landed_all(ZR.at[l], slot)
        before = identity
        for d in range(nz - 1, 0, -1):
            piece = jnp.concatenate([ZR[l, d - 1, j] for j in range(n)], axis=0)
            before = jnp.where(d <= z, chained(before, piece), before)
        return chained(before, within)

    def second_half(l, starts, incoming):
        turned = swapped(incoming)
        for jp in range(pairs):
            start_run, start_h = starts[jp]
            carry = start_h + start_run * halves(turned[2 * jp:2 * jp + 1], incoming[2 * jp + 1:2 * jp + 2])
            out_gain = PAR[l, q, jp][5:6]
            for k in range(steps):
                rows = pl.ds(k, ROWS, stride=steps)
                MIX[jp, rows, :] = (LOC[jp, k] + ACU[jp, k] * carry) * GEL[jp, rows, :] * out_gain
            MX[l, q, :, jp * LANE:(jp + 1) * LANE] = MIX[jp].astype(bf16)
        return [put(MX.at[l, q], MX.at[l, q], s, tp_of(c, p, (q + d) % n)) for d in near]

    def update(l, emit):
        squares = jnp.zeros((tq, LANE), f32)
        for qq in range(n):
            for jp in range(pairs):
                v = MX[l, qq, :, jp * LANE:(jp + 1) * LANE].astype(f32) / PAR[l, qq, jp][5:6]
                squares = squares + v * v
        scale = lax.rsqrt(jnp.sum(squares, axis=1, keepdims=True) * (1.0 / (n * C)) + EPS)
        mixed = jnp.concatenate([MX[l, qq] for qq in range(n)], axis=1)
        for jp in range(pairs):
            w = jnp.concatenate(
                [WO[l, 2 * jp].reshape(n * C, LANE), WO[l, 2 * jp + 1].reshape(n * C, LANE)], axis=1)
            up = jnp.dot(mixed, w, preferred_element_type=f32) * scale
            for j in (0, 1):
                at = tp_of(c, 2 * jp + j, q)
                emit(2 * jp + j, (XM[l, at].astype(f32) + up[:, j * LANE:(j + 1) * LANE]).astype(bf16))

    par_in = [put(PAR.at[:, q], PAR.at[:, q], s, tp_of(c, p, (q + d) % n)) for d in near]
    landed(t_b)
    l1_in = [far_first(1) if half > 1 else []]
    ring_step(half)
    if half == 1:
        l1_in = [far_first(1)]
    o_in = [spread_o(0), None]
    norm(0)
    landed_all(WX.at[0, 0:n - 1, :, 0], same)
    landed_all(WX.at[0, :, :, 0], other)
    landed(l1_in[0])
    l1_in.append(near_next(1))
    start = first_half(0)
    x_in = []
    cut = 3 * nt // 4

    def send_x():
        landed(l1_in[1])
        x_in.extend(spread_x(1, 0, cut))

    def send_o():
        o_in[1] = spread_o(1)

    incoming = prefix(0, send_x)
    gathered = second_half(0, start, incoming)
    x_in.extend(spread_x(1, cut, nt))
    landed(par_in)
    landed(o_in[0])
    landed(gathered)

    def keep_stream(j, v):
        XM[1, tp_of(c, j, q)] = v

    update(0, keep_stream)
    gathered = []
    for d in near:
        for j in range(n):
            ref = XM.at[1, tp_of(c, j, q)]
            gathered.append(put(ref, ref, s, tp_of(c, p, (q + d) % n)))
    rim1 = next(numbers)
    e, pp = (p + 1) // n, (p + 1) % n
    for j in range(n):
        at = tp_of(c, j, q)
        for qq in range(n):
            put(XM.at[1, at, tq - RIM:tq], XH.at[1, at], (s + e) % ns, tp_of((c + e) % 2, pp, qq), rim1)
    landed(gathered)
    landed_all(XH.at[1], rim1)
    norm(1)
    landed(x_in)
    start = first_half(1)
    incoming = prefix(1, send_o)
    gathered = second_half(1, start, incoming)
    landed(o_in[1])
    landed(gathered)

    def keep_last(j, v):
        FS[j] = v

    update(1, keep_last)
    last = [put(FS.at[(p + d) % n], OB.at[p], s, tp_of(c, (p + d) % n, q)) for d in near]
    OB[p] = FS[p]
    landed(last)
    for k in range(n):
        out[k * tq:(k + 1) * tq] = OB[k]
    for cp in sent:
        cp.wait_send()
    for cp, k in rim_sends:
        @pl.when(p != k)
        def _():
            cp.wait_send()


def body(tokens, mix_gain, x_weight, gate_weight, conv_taps, a_maps, i_maps, decay_rate, pace, jumps,
         out_gain, out_weight):
    nt = lax.axis_size("tp")
    n = int(round(nt ** 0.5))
    tq = tokens.shape[0] // n
    C = n * HEAD
    D = nt * LANE
    lines = (-1, LANE)
    vmem = pl.BlockSpec(memory_space=pltpu.VMEM)
    xr, orr = x_weight.shape[1], out_weight.shape[1]
    scratch = [
        pltpu.VMEM((LAYERS, xr, LANE), bf16),
        pltpu.VMEM((LAYERS, HEAD, LANE), bf16),
        pltpu.VMEM((LAYERS, ROWS, LANE), f32),
        pltpu.VMEM((2, n * tq, LANE), f32),
        pltpu.VMEM((LAYERS, n, nt, 2, xr, LANE), bf16),
        pltpu.VMEM((LAYERS, n, n, n, 2, orr, LANE), bf16),
        pltpu.VMEM((n, LAYERS, HEAD, LANE), bf16),
        pltpu.VMEM((n, LAYERS, ROWS, LANE), f32),
        pltpu.VMEM((LAYERS, nt, tq, LANE), bf16),
        pltpu.VMEM((LAYERS, nt, RIM, LANE), bf16),
        pltpu.VMEM((RIM + tq, D), bf16),
        pltpu.VMEM((n // 2, RIM + tq, LANE), f32),
        pltpu.VMEM((n // 2, tq, LANE), f32),
        pltpu.VMEM((LAYERS, n // 2, LANE, 2 * LANE), bf16),
        pltpu.VMEM((LAYERS, n, n // 2, ROWS, LANE), f32),
        pltpu.VMEM((n // 2, tq, LANE), f32),
        pltpu.VMEM((n // 2, tq, LANE), f32),
        pltpu.VMEM((n // 2, tq // ROWS, ROWS, LANE), f32),
        pltpu.VMEM((n // 2, tq // ROWS, ROWS, LANE), f32),
        pltpu.VMEM((n // 2, tq, LANE), f32),
        pltpu.VMEM((LAYERS, n, tq, C), bf16),
        pltpu.VMEM((LAYERS, n, 1, LANE), f32),
        pltpu.VMEM((LAYERS, 2, n, n, 1, LANE), f32),
        pltpu.VMEM((LAYERS, n, 1, LANE), f32),
        pltpu.VMEM((LAYERS, nt - 1, n, 1, LANE), f32),
        pltpu.VMEM((n, tq, LANE), bf16),
        pltpu.VMEM((n, tq, LANE), bf16),
        pltpu.SemaphoreType.DMA,
        pltpu.SemaphoreType.DMA((320,)),
    ]
    return pl.pallas_call(
        functools.partial(kernel, n, tq),
        out_shape=jax.ShapeDtypeStruct(tokens.shape, bf16),
        in_specs=[vmem] * 12,
        out_specs=vmem,
        scratch_shapes=scratch,
        compiler_params=pltpu.CompilerParams(collective_id=0, has_side_effects=True, vmem_limit_bytes=56 * 1024 * 1024),
    )(tokens, mix_gain, x_weight, gate_weight, out_weight, conv_taps, a_maps, i_maps, decay_rate, out_gain,
      pace.reshape(lines), jumps.reshape(lines))


def solution(mesh):
    in_specs = (
        P("sp", "tp"),
        P(),
        P(None, "sp", "tp"),
        P(None, "sp", "tp"),
        P(None, None, "tp"),
        P(None, "tp", None, None),
        P(None, "tp", None, None),
        P(None, "tp"),
        P("sp"),
        P("sp"),
        P(None, "tp"),
        P(None, "sp", "tp"),
    )
    return jax.shard_map(body, mesh=mesh, in_specs=in_specs, out_specs=P("sp", "tp"), check_vma=False)
```

```python
import functools

import jax
import jax.numpy as jnp
from jax import lax
from jax.experimental import pallas as pl
from jax.experimental.pallas import tpu as pltpu
from jax.sharding import PartitionSpec as P

HEAD = 64
WIDTH = 4
LAYERS = 2
EPS = 1e-06
GATE_C = 8.0
RIM = 16
LANE = 128
ROWS = 8

f32 = jnp.float32
bf16 = jnp.bfloat16


def swapped(x):
    return pltpu.roll(x, HEAD, 1)


def lower_half(shape):
    return lax.broadcasted_iota(jnp.int32, shape, len(shape) - 1) < HEAD


def halves(first, second):
    return jnp.where(lower_half(first.shape), first, second)


def chained(first, second):
    low = lower_half(second.shape)
    return jnp.where(low, second, swapped(second)) * first + jnp.where(low, 0.0, second)


def gelu(x):
    return 0.5 * x * (1.0 + jnp.tanh(0.7978845608028654 * (x + 0.044715 * (x * x * x))))


def one_minus_exp(y, decay):
    series = jnp.ones_like(y)
    for k in range(8, 1, -1):
        series = 1.0 - (y * (1.0 / k)) * series
    return jnp.where(y < 0.5, y * series, 1.0 - decay * decay)


def kernel(n, tq, tok, gain, xw, gw, wo, taps, am, im, rate, og, pace, jumps, out,
           WXG, MAPO, SMO, PJ, WX, WO, MAPS, SMALL, XM, XH, NRM, XR, GEL, BD, PAR, AS, BS, LOC, ACU, MIX, MX,
           PO, PR, ZO, ZR, FS, OB, send, recv):
    nt, nz, ns = n * n, n * n, 2 * n * n
    C = n * HEAD
    pairs = n // 2
    D = nt * LANE
    steps = tq // ROWS
    s, tp = lax.axis_index("sp"), lax.axis_index("tp")
    c, z = s % 2, s // 2
    a, b = z // n, z % n
    y, x = tp // n, tp % n
    p, q = x + c * (y - x), y + c * (x - y)

    def tp_of(core, pp, qq):
        return (qq * n + pp) + core * ((pp * n + qq) - (qq * n + pp))

    sent = []
    numbers = iter(range(10000))

    def put(src, dst, sp_to, tp_to, slot=None):
        slot = next(numbers) if slot is None else slot
        cp = pltpu.make_async_remote_copy(
            src_ref=src, dst_ref=dst, send_sem=send, recv_sem=recv.at[slot],
            device_id={"sp": sp_to, "tp": tp_to}, device_id_type=pl.DeviceIdType.MESH)
        cp.start()
        sent.append(cp)
        return cp

    def landed(copies):
        for cp in copies:
            cp.wait_recv()

    def landed_all(ref, slot):
        pltpu.make_async_copy(ref, ref, recv.at[slot]).wait()

    near = range(1, n)
    reach = min(4, nz // 2)
    half = nz // 2 // reach
    across = 1 - c

    barrier = pltpu.get_barrier_semaphore()

    def greet(sp_to, tp_to):
        pl.semaphore_signal(barrier, inc=1, device_id={"sp": sp_to, "tp": tp_to},
                            device_id_type=pl.DeviceIdType.MESH)

    def zat(d, core=None):
        return ((z + d + nz) % nz) * 2 + (c if core is None else core)

    zs = sorted({d % nz for d in range(-reach, reach + 1)} - {0})
    for d in near:
        greet(s, tp_of(c, (p + d) % n, q))
        greet(s, tp_of(c, p, (q + d) % n))
    for d in range(n):
        greet(z * 2 + across, tp_of(across, q, d))
    for d in zs:
        greet(zat(d), tp)

    @pl.when((1 - c) * (1 - jnp.minimum(p, 1)) == 1)
    def _():
        for k in range(n):
            greet(zat(-1, 1), tp_of(1, q, k))

    for l in range(LAYERS):
        WXG[l] = jnp.concatenate([xw[l], gw[l]], axis=1)
        MAPO[l] = jnp.concatenate([am[l, 0], im[l, 0]], axis=1)
        rows = jnp.concatenate(
            [taps[l].astype(f32), rate[l:l + 1], og[l:l + 1].astype(f32), jnp.ones((2, HEAD), f32)], axis=0)
        SMO[l] = jnp.concatenate([rows, rows], axis=1)
    for i, ref in enumerate((pace, jumps)):
        for r in range(n * tq // LANE):
            PJ[i, r * LANE:(r + 1) * LANE] = jnp.transpose(jnp.broadcast_to(ref[r:r + 1], (LANE, LANE)))
    pl.semaphore_wait(barrier, 2 * (n - 1) + n + len(zs) + c)

    def x_piece(l, o):
        return WX.at[l, p, o, c]

    def o_piece(l, o):
        i, k = o // n, o % n
        return WO.at[l, p, i + c * (k - i), k + c * (i - k), c]

    def hops(k):
        for sign, i in ((1, 0), (-1, reach)):
            for j in range(1, reach + 1):
                if sign == 1 or j < reach or k < half - 1:
                    yield sign, j, 2 * reach * k + i + j - 1

    def ring_numbers():
        return [next(numbers) for _ in range(2 * reach * half)]

    def ring_send(piece, own, l, k, slots):
        for sign, j, i in hops(k):
            dst = piece(l, (z - sign * reach * k + nz) % nz)
            put(own if k == 0 else dst, dst, zat(sign * j), tp, slots[i])

    def ring_land(piece, l, k, slots):
        got = []
        for sign, j, i in hops(k):
            o = (z - sign * (reach * k + j) + nz) % nz
            landed_all(piece(l, o), slots[i])
            got.append(o)
        return got

    same, other = next(numbers), next(numbers)

    def spread(o, src=None):
        ref = WX.at[0, p, o, c]
        src = ref if src is None else src
        for d in near:
            put(src, ref, s, tp_of(c, (p + d) % n, q), same)
        for d in range(n):
            put(src, WX.at[0, q, o, c], z * 2 + across, tp_of(across, (q + d) % n, p), other)

    def spread_x(l, first, last):
        part = pl.ds(first, last - first)
        made = [put(WX.at[l, p, part, c], WX.at[l, p, part, c], s, tp_of(c, (p + d) % n, q)) for d in near]
        for d in range(n):
            made.append(put(WX.at[l, p, part, c], WX.at[l, q, part, c], z * 2 + across,
                            tp_of(across, (q + d) % n, p)))
        return made

    def far_first(l):
        made = []
        for d in near:
            to = (((a + d) % n) * n + b) * 2 + c
            made.append(put(WXG.at[l], x_piece(l, z), to, tp))
            made.append(put(wo.at[l], o_piece(l, z), to, tp))
        return made

    def near_next(l):
        made = []
        for piece in (x_piece, o_piece):
            for d in near:
                for k in range(n):
                    ref = piece(l, k * n + b)
                    made.append(put(ref, ref, (a * n + (b + d) % n) * 2 + c, tp))
        return made

    def spread_o(l):
        made = [put(WO.at[l, p, :, :, c], WO.at[l, p, :, :, c], s, tp_of(c, (p + d) % n, q)) for d in near]
        for d in range(n):
            for k in range(n):
                made.append(put(WO.at[l, p, k, :, c], WO.at[l, q, :, k, c], z * 2 + across,
                                tp_of(across, (q + d) % n, p)))
        return made

    firsts = {(kind, 0): ring_numbers() for kind in "xo"}

    own = pl.ds(pl.multiple_of(p * tq, tq), tq)
    t_a = []
    for d in near:
        pp = (p + d) % n
        rows = pl.ds(pl.multiple_of(pp * tq, tq), tq)
        t_a.append(put(tok.at[rows], XM.at[0, tp], s, tp_of(c, pp, q)))
    rim0 = next(numbers)
    rim_sends = []
    for k in range(n - 1):
        src = tok.at[(k + 1) * tq - RIM:(k + 1) * tq]
        cp = pltpu.make_async_remote_copy(
            src_ref=src, dst_ref=XH.at[0, tp], send_sem=send, recv_sem=recv.at[rim0],
            device_id={"sp": s, "tp": tp_of(c, k + 1, q)}, device_id_type=pl.DeviceIdType.MESH)

        @pl.when(p != k + 1)
        def _():
            cp.start()

        @pl.when(p == k + 1)
        def _():
            XH[0, tp] = src[...]
        rim_sends.append((cp, k + 1))
    put(tok.at[n * tq - RIM:n * tq], XH.at[0, tp], (s + 1) % ns, tp_of(across, 0, p), rim0)
    ring_send(x_piece, WXG.at[0], 0, 0, firsts["x", 0])
    spread(z, WXG.at[0])
    m_in = [put(MAPO, MAPS.at[p], s, tp_of(c, (p + d) % n, q)) for d in near]
    s_in = [put(SMO, SMALL.at[p], s, tp_of(c, (p + d) % n, q)) for d in near]
    ring_send(o_piece, wo.at[0], 0, 0, firsts["o", 0])

    XM[0, tp] = tok[own]
    for l in range(LAYERS):
        WX[l, p, z, c] = WXG[l]
        WO[l, p, a + c * (b - a), b + c * (a - b), c] = wo[l]
    MAPS[p] = MAPO[...]
    SMALL[p] = SMO[...]

    landed(t_a)

    @pl.when(p > 0)
    def _():
        landed_all(XH.at[0, :n - 1], rim0)

    @pl.when(p == 0)
    def _():
        landed_all(XH.at[0, :n], rim0)

    t_b = []
    for d in near:
        to = tp_of(c, p, (q + d) % n)
        t_b.append(put(tok.at[own], XM.at[0, tp], s, to))
        for e in near:
            ref = XM.at[0, tp_of(c, (p + e) % n, q)]
            t_b.append(put(ref, ref, s, to))
        for e in range(n):
            ref = XH.at[0, tp_of(c, (p + e) % n, q)]
            t_b.append(put(ref, ref, s, to))

    def ring_step(k):
        if k < half:
            got = ring_land(x_piece, 0, k - 1, firsts["x", 0])
            ring_send(x_piece, None, 0, k, firsts["x", 0])
        else:
            got = ring_land(x_piece, 0, half - 1, firsts["x", 0])
        for o in got:
            spread(o)
        ring_land(o_piece, 0, k - 1, firsts["o", 0])
        if k < half:
            ring_send(o_piece, None, 0, k, firsts["o", 0])

    for k in range(1, half):
        ring_step(k)

    landed(m_in)
    landed(s_in)
    for l in range(LAYERS):
        for jp in range(pairs):
            even = MAPS[2 * jp, l].astype(f32)
            odd = MAPS[2 * jp + 1, l].astype(f32)
            low = lower_half(even.shape)
            BD[l, jp, :HEAD, :LANE] = jnp.where(low, even, 0.0).astype(bf16)
            BD[l, jp, :HEAD, LANE:] = jnp.where(low, swapped(even), 0.0).astype(bf16)
            BD[l, jp, HEAD:, :LANE] = jnp.where(low, 0.0, swapped(odd)).astype(bf16)
            BD[l, jp, HEAD:, LANE:] = jnp.where(low, 0.0, odd).astype(bf16)
            PAR[l, q, jp] = halves(SMALL[2 * jp, l], SMALL[2 * jp + 1, l])

    def norm_rows(l, block, row):
        total = jnp.zeros((RIM, LANE), f32)
        for t in range(nt):
            v = block(t).astype(f32)
            total = total + v * v
        r = lax.rsqrt(jnp.sum(total, axis=1, keepdims=True) * (1.0 / D) + EPS)
        for t in range(nt):
            cols = slice(t * LANE, (t + 1) * LANE)
            g = gain[l:l + 1, cols].astype(f32)
            NRM[pl.ds(row, RIM), cols] = (block(t).astype(f32) * r * g).astype(bf16)

    def norm(l):
        norm_rows(l, lambda t: XH[l, t], 0)

        @pl.loop(0, tq // RIM)
        def _(i):
            row = pl.multiple_of(i * RIM, RIM)
            norm_rows(l, lambda t: XM[l, t, pl.ds(row, RIM), :], pl.multiple_of(row + RIM, RIM))

    def first_half(l):
        keep = jnp.minimum(s + p, 1).astype(f32)
        normed = NRM[...]
        speed = PJ[0, own, :]
        jump = PJ[1, own, :]
        for jp in range(pairs):
            w = jnp.concatenate(
                [WX[l, 2 * jp].reshape(D, LANE), WX[l, 2 * jp + 1].reshape(D, LANE)], axis=1)
            pr = jnp.dot(normed, w, preferred_element_type=f32).astype(bf16).astype(f32)
            left, right = pr[:, :LANE], pr[:, LANE:]
            xr = halves(left, swapped(right))
            XR[jp, :RIM] = xr[:RIM] * keep
            XR[jp, RIM:] = xr[RIM:]
            GEL[jp] = gelu(halves(swapped(left), right)[RIM:])
            par = PAR[l, q, jp]
            conv = jnp.zeros((tq, LANE), f32)
            for k in range(WIDTH):
                conv = conv + par[k:k + 1] * XR[jp, pl.ds(RIM - WIDTH + 1 + k, tq), :]
            xc = conv.astype(bf16)
            gates = jnp.dot(xc, BD[l, jp], preferred_element_type=f32)
            r = jax.nn.sigmoid(gates[:, :LANE])
            gin = jax.nn.sigmoid(gates[:, LANE:])
            log_a = -GATE_C * r * par[4:5] * speed + jump
            decay = jnp.exp(log_a)
            AS[jp] = decay
            BS[jp] = jnp.sqrt(one_minus_exp(-2.0 * log_a, decay)) * gin * xc.astype(f32)
        starts = []
        for jp in range(pairs):
            run = h = None
            for k in range(steps):
                ak = AS[jp, pl.ds(k, ROWS, stride=steps), :]
                bk = BS[jp, pl.ds(k, ROWS, stride=steps), :]
                h = bk if k == 0 else ak * h + bk
                run = ak if k == 0 else ak * run
                LOC[jp, k], ACU[jp, k] = h, run
            row = lax.broadcasted_iota(jnp.int32, (ROWS, LANE), 0)
            for d in (1, 2, 4):
                before = row >= d
                h = run * jnp.where(before, pltpu.roll(h, d, 0), 0.0) + h
                run = run * jnp.where(before, pltpu.roll(run, d, 0), 1.0)
            av, sv = run[ROWS - 1:], h[ROWS - 1:]
            PO[l, 2 * jp] = halves(av, swapped(sv))
            PO[l, 2 * jp + 1] = halves(swapped(av), sv)
            starts.append((jnp.where(row >= 1, pltpu.roll(run, 1, 0), 1.0),
                           jnp.where(row >= 1, pltpu.roll(h, 1, 0), 0.0)))
        return starts

    def prefix(l, meanwhile):
        made = []
        for d in near:
            made.append(put(PO.at[l], PR.at[l, c, p], s, tp_of(c, (p + d) % n, q)))
        slot = next(numbers)
        for k in range(n):
            for pp in range(n):
                put(PO.at[l, k], PR.at[l, c, p, q], z * 2 + 1 - c, tp_of(1 - c, pp, k), slot)
        for j in range(n):
            PR[l, c, p, j] = PO[l, j]
        landed(made)
        landed_all(PR.at[l, 1 - c], slot)
        identity = jnp.where(lower_half((n, LANE)), 1.0, 0.0)
        total = within = identity
        mine = c * n + p
        for i in range(2 * n):
            piece = jnp.concatenate([PR[l, i // n, i % n, j] for j in range(n)], axis=0)
            within = jnp.where(i < mine, chained(within, piece), within)
            total = chained(total, piece)
        for j in range(n):
            ZO[l, j] = total[j:j + 1]
        slot = next(numbers)
        for d in range(1, nz):
            put(ZO.at[l], ZR.at[l, d - 1], ((z + d) % nz) * 2 + c, tp, slot)
        meanwhile()
        landed_all(ZR.at[l], slot)
        before = identity
        for d in range(nz - 1, 0, -1):
            piece = jnp.concatenate([ZR[l, d - 1, j] for j in range(n)], axis=0)
            before = jnp.where(d <= z, chained(before, piece), before)
        return chained(before, within)

    def second_half(l, starts, incoming):
        turned = swapped(incoming)
        for jp in range(pairs):
            start_run, start_h = starts[jp]
            carry = start_h + start_run * halves(turned[2 * jp:2 * jp + 1], incoming[2 * jp + 1:2 * jp + 2])
            out_gain = PAR[l, q, jp][5:6]
            for k in range(steps):
                rows = pl.ds(k, ROWS, stride=steps)
                MIX[jp, rows, :] = (LOC[jp, k] + ACU[jp, k] * carry) * GEL[jp, rows, :] * out_gain
            MX[l, q, :, jp * LANE:(jp + 1) * LANE] = MIX[jp].astype(bf16)
        return [put(MX.at[l, q], MX.at[l, q], s, tp_of(c, p, (q + d) % n)) for d in near]

    def update(l, emit):
        squares = jnp.zeros((tq, LANE), f32)
        for qq in range(n):
            for jp in range(pairs):
                v = MX[l, qq, :, jp * LANE:(jp + 1) * LANE].astype(f32) / PAR[l, qq, jp][5:6]
                squares = squares + v * v
        scale = lax.rsqrt(jnp.sum(squares, axis=1, keepdims=True) * (1.0 / (n * C)) + EPS)
        mixed = jnp.concatenate([MX[l, qq] for qq in range(n)], axis=1)
        for jp in range(pairs):
            w = jnp.concatenate(
                [WO[l, 2 * jp].reshape(n * C, LANE), WO[l, 2 * jp + 1].reshape(n * C, LANE)], axis=1)
            up = jnp.dot(mixed, w, preferred_element_type=f32) * scale
            for j in (0, 1):
                at = tp_of(c, 2 * jp + j, q)
                emit(2 * jp + j, (XM[l, at].astype(f32) + up[:, j * LANE:(j + 1) * LANE]).astype(bf16))

    par_in = [put(PAR.at[:, q], PAR.at[:, q], s, tp_of(c, p, (q + d) % n)) for d in near]
    l1_in = [far_first(1)]
    landed(t_b)
    ring_step(half)
    o_in = [spread_o(0), None]
    norm(0)
    landed(l1_in[0])
    l1_in.append(near_next(1))
    landed_all(WX.at[0, 0:n - 1, :, 0], same)
    landed_all(WX.at[0, :, :, 0], other)
    start = first_half(0)
    x_in = []
    cut = 3 * nt // 4

    def send_x():
        landed(l1_in[1])
        x_in.extend(spread_x(1, 0, cut))

    def send_o():
        o_in[1] = spread_o(1)

    incoming = prefix(0, send_x)
    gathered = second_half(0, start, incoming)
    landed(par_in)
    landed(o_in[0])
    landed(gathered)

    def keep_stream(j, v):
        XM[1, tp_of(c, j, q)] = v

    update(0, keep_stream)
    gathered = []
    for d in near:
        for j in range(n):
            ref = XM.at[1, tp_of(c, j, q)]
            gathered.append(put(ref, ref, s, tp_of(c, p, (q + d) % n)))
    rim1 = next(numbers)
    e, pp = (p + 1) // n, (p + 1) % n
    for j in range(n):
        at = tp_of(c, j, q)
        for qq in range(n):
            put(XM.at[1, at, tq - RIM:tq], XH.at[1, at], (s + e) % ns, tp_of((c + e) % 2, pp, qq), rim1)
    x_in.extend(spread_x(1, cut, nt))
    landed(gathered)
    landed_all(XH.at[1], rim1)
    norm(1)
    landed(x_in)
    start = first_half(1)
    incoming = prefix(1, send_o)
    gathered = second_half(1, start, incoming)
    landed(o_in[1])
    landed(gathered)

    def keep_last(j, v):
        FS[j] = v

    update(1, keep_last)
    last = [put(FS.at[(p + d) % n], OB.at[p], s, tp_of(c, (p + d) % n, q)) for d in near]
    OB[p] = FS[p]
    landed(last)
    for k in range(n):
        out[k * tq:(k + 1) * tq] = OB[k]
    for cp in sent:
        cp.wait_send()
    for cp, k in rim_sends:
        @pl.when(p != k)
        def _():
            cp.wait_send()


def body(tokens, mix_gain, x_weight, gate_weight, conv_taps, a_maps, i_maps, decay_rate, pace, jumps,
         out_gain, out_weight):
    nt = lax.axis_size("tp")
    n = int(round(nt ** 0.5))
    tq = tokens.shape[0] // n
    C = n * HEAD
    D = nt * LANE
    lines = (-1, LANE)
    vmem = pl.BlockSpec(memory_space=pltpu.VMEM)
    xr, orr = x_weight.shape[1], out_weight.shape[1]
    scratch = [
        pltpu.VMEM((LAYERS, xr, LANE), bf16),
        pltpu.VMEM((LAYERS, HEAD, LANE), bf16),
        pltpu.VMEM((LAYERS, ROWS, LANE), f32),
        pltpu.VMEM((2, n * tq, LANE), f32),
        pltpu.VMEM((LAYERS, n, nt, 2, xr, LANE), bf16),
        pltpu.VMEM((LAYERS, n, n, n, 2, orr, LANE), bf16),
        pltpu.VMEM((n, LAYERS, HEAD, LANE), bf16),
        pltpu.VMEM((n, LAYERS, ROWS, LANE), f32),
        pltpu.VMEM((LAYERS, nt, tq, LANE), bf16),
        pltpu.VMEM((LAYERS, nt, RIM, LANE), bf16),
        pltpu.VMEM((RIM + tq, D), bf16),
        pltpu.VMEM((n // 2, RIM + tq, LANE), f32),
        pltpu.VMEM((n // 2, tq, LANE), f32),
        pltpu.VMEM((LAYERS, n // 2, LANE, 2 * LANE), bf16),
        pltpu.VMEM((LAYERS, n, n // 2, ROWS, LANE), f32),
        pltpu.VMEM((n // 2, tq, LANE), f32),
        pltpu.VMEM((n // 2, tq, LANE), f32),
        pltpu.VMEM((n // 2, tq // ROWS, ROWS, LANE), f32),
        pltpu.VMEM((n // 2, tq // ROWS, ROWS, LANE), f32),
        pltpu.VMEM((n // 2, tq, LANE), f32),
        pltpu.VMEM((LAYERS, n, tq, C), bf16),
        pltpu.VMEM((LAYERS, n, 1, LANE), f32),
        pltpu.VMEM((LAYERS, 2, n, n, 1, LANE), f32),
        pltpu.VMEM((LAYERS, n, 1, LANE), f32),
        pltpu.VMEM((LAYERS, nt - 1, n, 1, LANE), f32),
        pltpu.VMEM((n, tq, LANE), bf16),
        pltpu.VMEM((n, tq, LANE), bf16),
        pltpu.SemaphoreType.DMA,
        pltpu.SemaphoreType.DMA((320,)),
    ]
    return pl.pallas_call(
        functools.partial(kernel, n, tq),
        out_shape=jax.ShapeDtypeStruct(tokens.shape, bf16),
        in_specs=[vmem] * 12,
        out_specs=vmem,
        scratch_shapes=scratch,
        compiler_params=pltpu.CompilerParams(collective_id=0, has_side_effects=True, vmem_limit_bytes=56 * 1024 * 1024),
    )(tokens, mix_gain, x_weight, gate_weight, out_weight, conv_taps, a_maps, i_maps, decay_rate, out_gain,
      pace.reshape(lines), jumps.reshape(lines))


def solution(mesh):
    in_specs = (
        P("sp", "tp"),
        P(),
        P(None, "sp", "tp"),
        P(None, "sp", "tp"),
        P(None, None, "tp"),
        P(None, "tp", None, None),
        P(None, "tp", None, None),
        P(None, "tp"),
        P("sp"),
        P("sp"),
        P(None, "tp"),
        P(None, "sp", "tp"),
    )
    return jax.shard_map(body, mesh=mesh, in_specs=in_specs, out_specs=P("sp", "tp"), check_vma=False)
```

```python
import functools

import jax
import jax.numpy as jnp
from jax import lax
from jax.experimental import pallas as pl
from jax.experimental.pallas import tpu as pltpu
from jax.sharding import PartitionSpec as P

HEAD = 64
WIDTH = 4
LAYERS = 2
EPS = 1e-06
GATE_C = 8.0
RIM = 16
LANE = 128
ROWS = 8

f32 = jnp.float32
bf16 = jnp.bfloat16


def swapped(x):
    return pltpu.roll(x, HEAD, 1)


def lower_half(shape):
    return lax.broadcasted_iota(jnp.int32, shape, len(shape) - 1) < HEAD


def halves(first, second):
    return jnp.where(lower_half(first.shape), first, second)


def chained(first, second):
    low = lower_half(second.shape)
    return jnp.where(low, second, swapped(second)) * first + jnp.where(low, 0.0, second)


def gelu(x):
    return 0.5 * x * (1.0 + jnp.tanh(0.7978845608028654 * (x + 0.044715 * (x * x * x))))


def one_minus_exp(y, decay):
    series = jnp.ones_like(y)
    for k in range(8, 1, -1):
        series = 1.0 - (y * (1.0 / k)) * series
    return jnp.where(y < 0.5, y * series, 1.0 - decay * decay)


def kernel(n, tq, tok, gain, xw, gw, wo, taps, am, im, rate, og, pace, jumps, out,
           WXG, MAPO, SMO, PJ, WX, WO, MAPS, SMALL, XM, XH, NRM, XR, GEL, BD, PAR, AS, BS, LOC, ACU, MIX, MX,
           PO, PR, ZO, ZR, FS, OB, send, recv):
    nt, nz, ns = n * n, n * n, 2 * n * n
    C = n * HEAD
    pairs = n // 2
    D = nt * LANE
    steps = tq // ROWS
    s, tp = lax.axis_index("sp"), lax.axis_index("tp")
    c, z = s % 2, s // 2
    a, b = z // n, z % n
    y, x = tp // n, tp % n
    p, q = x + c * (y - x), y + c * (x - y)

    def tp_of(core, pp, qq):
        return (qq * n + pp) + core * ((pp * n + qq) - (qq * n + pp))

    sent = []
    numbers = iter(range(10000))

    def put(src, dst, sp_to, tp_to, slot=None):
        slot = next(numbers) if slot is None else slot
        cp = pltpu.make_async_remote_copy(
            src_ref=src, dst_ref=dst, send_sem=send, recv_sem=recv.at[slot],
            device_id={"sp": sp_to, "tp": tp_to}, device_id_type=pl.DeviceIdType.MESH)
        cp.start()
        sent.append(cp)
        return cp

    def landed(copies):
        for cp in copies:
            cp.wait_recv()

    def landed_all(ref, slot):
        pltpu.make_async_copy(ref, ref, recv.at[slot]).wait()

    near = range(1, n)
    reach = min(4, nz // 2)
    half = nz // 2 // reach
    across = 1 - c

    barrier = pltpu.get_barrier_semaphore()

    def greet(sp_to, tp_to):
        pl.semaphore_signal(barrier, inc=1, device_id={"sp": sp_to, "tp": tp_to},
                            device_id_type=pl.DeviceIdType.MESH)

    def zat(d, core=None):
        return ((z + d + nz) % nz) * 2 + (c if core is None else core)

    zs = sorted({d % nz for d in range(-reach, reach + 1)} - {0})
    for d in near:
        greet(s, tp_of(c, (p + d) % n, q))
        greet(s, tp_of(c, p, (q + d) % n))
    for d in range(n):
        greet(z * 2 + across, tp_of(across, q, d))
    for d in zs:
        greet(zat(d), tp)

    @pl.when((1 - c) * (1 - jnp.minimum(p, 1)) == 1)
    def _():
        for k in range(n):
            greet(zat(-1, 1), tp_of(1, q, k))

    for l in range(LAYERS):
        WXG[l] = jnp.concatenate([xw[l], gw[l]], axis=1)
        MAPO[l] = jnp.concatenate([am[l, 0], im[l, 0]], axis=1)
        rows = jnp.concatenate(
            [taps[l].astype(f32), rate[l:l + 1], og[l:l + 1].astype(f32), jnp.ones((2, HEAD), f32)], axis=0)
        SMO[l] = jnp.concatenate([rows, rows], axis=1)
    for i, ref in enumerate((pace, jumps)):
        for r in range(n * tq // LANE):
            PJ[i, r * LANE:(r + 1) * LANE] = jnp.transpose(jnp.broadcast_to(ref[r:r + 1], (LANE, LANE)))
    pl.semaphore_wait(barrier, 2 * (n - 1) + n + len(zs) + c)

    def x_piece(l, o):
        return WX.at[l, p, o, c]

    def o_piece(l, o):
        i, k = o // n, o % n
        return WO.at[l, p, i + c * (k - i), k + c * (i - k), c]

    def hops(k):
        for sign, i in ((1, 0), (-1, reach)):
            for j in range(1, reach + 1):
                if sign == 1 or j < reach or k < half - 1:
                    yield sign, j, 2 * reach * k + i + j - 1

    def ring_numbers():
        return [next(numbers) for _ in range(2 * reach * half)]

    def ring_send(piece, own, l, k, slots):
        for sign, j, i in hops(k):
            dst = piece(l, (z - sign * reach * k + nz) % nz)
            put(own if k == 0 else dst, dst, zat(sign * j), tp, slots[i])

    def ring_land(piece, l, k, slots):
        got = []
        for sign, j, i in hops(k):
            o = (z - sign * (reach * k + j) + nz) % nz
            landed_all(piece(l, o), slots[i])
            got.append(o)
        return got

    same, other = next(numbers), next(numbers)

    def spread(o, src=None):
        ref = WX.at[0, p, o, c]
        src = ref if src is None else src
        for d in near:
            put(src, ref, s, tp_of(c, (p + d) % n, q), same)
        for d in range(n):
            put(src, WX.at[0, q, o, c], z * 2 + across, tp_of(across, (q + d) % n, p), other)

    def spread_x(l, first, last):
        part = pl.ds(first, last - first)
        made = [put(WX.at[l, p, part, c], WX.at[l, p, part, c], s, tp_of(c, (p + d) % n, q)) for d in near]
        for d in range(n):
            made.append(put(WX.at[l, p, part, c], WX.at[l, q, part, c], z * 2 + across,
                            tp_of(across, (q + d) % n, p)))
        return made

    def far_first(l):
        made = []
        for d in near:
            to = (((a + d) % n) * n + b) * 2 + c
            made.append(put(WXG.at[l], x_piece(l, z), to, tp))
            made.append(put(wo.at[l], o_piece(l, z), to, tp))
        return made

    def near_next(l):
        made = []
        for piece in (x_piece, o_piece):
            for d in near:
                for k in range(n):
                    ref = piece(l, k * n + b)
                    made.append(put(ref, ref, (a * n + (b + d) % n) * 2 + c, tp))
        return made

    def spread_o(l):
        made = [put(WO.at[l, p, :, :, c], WO.at[l, p, :, :, c], s, tp_of(c, (p + d) % n, q)) for d in near]
        for d in range(n):
            for k in range(n):
                made.append(put(WO.at[l, p, k, :, c], WO.at[l, q, :, k, c], z * 2 + across,
                                tp_of(across, (q + d) % n, p)))
        return made

    firsts = {(kind, 0): ring_numbers() for kind in "xo"}

    own = pl.ds(pl.multiple_of(p * tq, tq), tq)
    t_a = []
    for d in near:
        pp = (p + d) % n
        rows = pl.ds(pl.multiple_of(pp * tq, tq), tq)
        t_a.append(put(tok.at[rows], XM.at[0, tp], s, tp_of(c, pp, q)))
    rim0 = next(numbers)
    rim_sends = []
    for k in range(n - 1):
        src = tok.at[(k + 1) * tq - RIM:(k + 1) * tq]
        cp = pltpu.make_async_remote_copy(
            src_ref=src, dst_ref=XH.at[0, tp], send_sem=send, recv_sem=recv.at[rim0],
            device_id={"sp": s, "tp": tp_of(c, k + 1, q)}, device_id_type=pl.DeviceIdType.MESH)

        @pl.when(p != k + 1)
        def _():
            cp.start()

        @pl.when(p == k + 1)
        def _():
            XH[0, tp] = src[...]
        rim_sends.append((cp, k + 1))
    put(tok.at[n * tq - RIM:n * tq], XH.at[0, tp], (s + 1) % ns, tp_of(across, 0, p), rim0)
    ring_send(x_piece, WXG.at[0], 0, 0, firsts["x", 0])
    spread(z, WXG.at[0])
    m_in = [put(MAPO, MAPS.at[p], s, tp_of(c, (p + d) % n, q)) for d in near]
    s_in = [put(SMO, SMALL.at[p], s, tp_of(c, (p + d) % n, q)) for d in near]
    ring_send(o_piece, wo.at[0], 0, 0, firsts["o", 0])

    XM[0, tp] = tok[own]
    for l in range(LAYERS):
        WX[l, p, z, c] = WXG[l]
        WO[l, p, a + c * (b - a), b + c * (a - b), c] = wo[l]
    MAPS[p] = MAPO[...]
    SMALL[p] = SMO[...]

    landed(t_a)
    t_b = []
    for d in near:
        to = tp_of(c, p, (q + d) % n)
        t_b.append(put(tok.at[own], XM.at[0, tp], s, to))
        for e in near:
            ref = XM.at[0, tp_of(c, (p + e) % n, q)]
            t_b.append(put(ref, ref, s, to))

    @pl.when(p > 0)
    def _():
        landed_all(XH.at[0, :n - 1], rim0)

    @pl.when(p == 0)
    def _():
        landed_all(XH.at[0, :n], rim0)

    for d in near:
        for e in range(n):
            ref = XH.at[0, tp_of(c, (p + e) % n, q)]
            t_b.append(put(ref, ref, s, tp_of(c, p, (q + d) % n)))

    def ring_step(k):
        if k < half:
            got = ring_land(x_piece, 0, k - 1, firsts["x", 0])
            ring_send(x_piece, None, 0, k, firsts["x", 0])
        else:
            got = ring_land(x_piece, 0, half - 1, firsts["x", 0])
        for o in got:
            spread(o)
        ring_land(o_piece, 0, k - 1, firsts["o", 0])
        if k < half:
            ring_send(o_piece, None, 0, k, firsts["o", 0])

    for k in range(1, half):
        ring_step(k)

    landed(m_in)
    landed(s_in)
    for l in range(LAYERS):
        for jp in range(pairs):
            even = MAPS[2 * jp, l].astype(f32)
            odd = MAPS[2 * jp + 1, l].astype(f32)
            low = lower_half(even.shape)
            BD[l, jp, :HEAD, :LANE] = jnp.where(low, even, 0.0).astype(bf16)
            BD[l, jp, :HEAD, LANE:] = jnp.where(low, swapped(even), 0.0).astype(bf16)
            BD[l, jp, HEAD:, :LANE] = jnp.where(low, 0.0, swapped(odd)).astype(bf16)
            BD[l, jp, HEAD:, LANE:] = jnp.where(low, 0.0, odd).astype(bf16)
            PAR[l, q, jp] = halves(SMALL[2 * jp, l], SMALL[2 * jp + 1, l])

    def norm_rows(l, block, row):
        total = jnp.zeros((RIM, LANE), f32)
        for t in range(nt):
            v = block(t).astype(f32)
            total = total + v * v
        r = lax.rsqrt(jnp.sum(total, axis=1, keepdims=True) * (1.0 / D) + EPS)
        for t in range(nt):
            cols = slice(t * LANE, (t + 1) * LANE)
            g = gain[l:l + 1, cols].astype(f32)
            NRM[pl.ds(row, RIM), cols] = (block(t).astype(f32) * r * g).astype(bf16)

    def norm(l):
        norm_rows(l, lambda t: XH[l, t], 0)

        @pl.loop(0, tq // RIM)
        def _(i):
            row = pl.multiple_of(i * RIM, RIM)
            norm_rows(l, lambda t: XM[l, t, pl.ds(row, RIM), :], pl.multiple_of(row + RIM, RIM))

    def first_half(l):
        keep = jnp.minimum(s + p, 1).astype(f32)
        normed = NRM[...]
        speed = PJ[0, own, :]
        jump = PJ[1, own, :]
        for jp in range(pairs):
            w = jnp.concatenate(
                [WX[l, 2 * jp].reshape(D, LANE), WX[l, 2 * jp + 1].reshape(D, LANE)], axis=1)
            pr = jnp.dot(normed, w, preferred_element_type=f32).astype(bf16).astype(f32)
            left, right = pr[:, :LANE], pr[:, LANE:]
            xr = halves(left, swapped(right))
            XR[jp, :RIM] = xr[:RIM] * keep
            XR[jp, RIM:] = xr[RIM:]
            GEL[jp] = gelu(halves(swapped(left), right)[RIM:])
            par = PAR[l, q, jp]
            conv = jnp.zeros((tq, LANE), f32)
            for k in range(WIDTH):
                conv = conv + par[k:k + 1] * XR[jp, pl.ds(RIM - WIDTH + 1 + k, tq), :]
            xc = conv.astype(bf16)
            gates = jnp.dot(xc, BD[l, jp], preferred_element_type=f32)
            r = jax.nn.sigmoid(gates[:, :LANE])
            gin = jax.nn.sigmoid(gates[:, LANE:])
            log_a = -GATE_C * r * par[4:5] * speed + jump
            decay = jnp.exp(log_a)
            AS[jp] = decay
            BS[jp] = jnp.sqrt(one_minus_exp(-2.0 * log_a, decay)) * gin * xc.astype(f32)
        starts = []
        for jp in range(pairs):
            run = h = None
            for k in range(steps):
                ak = AS[jp, pl.ds(k, ROWS, stride=steps), :]
                bk = BS[jp, pl.ds(k, ROWS, stride=steps), :]
                h = bk if k == 0 else ak * h + bk
                run = ak if k == 0 else ak * run
                LOC[jp, k], ACU[jp, k] = h, run
            row = lax.broadcasted_iota(jnp.int32, (ROWS, LANE), 0)
            for d in (1, 2, 4):
                before = row >= d
                h = run * jnp.where(before, pltpu.roll(h, d, 0), 0.0) + h
                run = run * jnp.where(before, pltpu.roll(run, d, 0), 1.0)
            av, sv = run[ROWS - 1:], h[ROWS - 1:]
            PO[l, 2 * jp] = halves(av, swapped(sv))
            PO[l, 2 * jp + 1] = halves(swapped(av), sv)
            starts.append((jnp.where(row >= 1, pltpu.roll(run, 1, 0), 1.0),
                           jnp.where(row >= 1, pltpu.roll(h, 1, 0), 0.0)))
        return starts

    def prefix(l, meanwhile):
        made = []
        for d in near:
            made.append(put(PO.at[l], PR.at[l, c, p], s, tp_of(c, (p + d) % n, q)))
        slot = next(numbers)
        for k in range(n):
            for pp in range(n):
                put(PO.at[l, k], PR.at[l, c, p, q], z * 2 + 1 - c, tp_of(1 - c, pp, k), slot)
        for j in range(n):
            PR[l, c, p, j] = PO[l, j]
        landed(made)
        landed_all(PR.at[l, 1 - c], slot)
        identity = jnp.where(lower_half((n, LANE)), 1.0, 0.0)
        total = within = identity
        mine = c * n + p
        for i in range(2 * n):
            piece = jnp.concatenate([PR[l, i // n, i % n, j] for j in range(n)], axis=0)
            within = jnp.where(i < mine, chained(within, piece), within)
            total = chained(total, piece)
        for j in range(n):
            ZO[l, j] = total[j:j + 1]
        slot = next(numbers)
        for d in range(1, nz):
            put(ZO.at[l], ZR.at[l, d - 1], ((z + d) % nz) * 2 + c, tp, slot)
        meanwhile()
        landed_all(ZR.at[l], slot)
        before = identity
        for d in range(nz - 1, 0, -1):
            piece = jnp.concatenate([ZR[l, d - 1, j] for j in range(n)], axis=0)
            before = jnp.where(d <= z, chained(before, piece), before)
        return chained(before, within)

    def second_half(l, starts, incoming):
        turned = swapped(incoming)
        for jp in range(pairs):
            start_run, start_h = starts[jp]
            carry = start_h + start_run * halves(turned[2 * jp:2 * jp + 1], incoming[2 * jp + 1:2 * jp + 2])
            out_gain = PAR[l, q, jp][5:6]
            for k in range(steps):
                rows = pl.ds(k, ROWS, stride=steps)
                MIX[jp, rows, :] = (LOC[jp, k] + ACU[jp, k] * carry) * GEL[jp, rows, :] * out_gain
            MX[l, q, :, jp * LANE:(jp + 1) * LANE] = MIX[jp].astype(bf16)
        return [put(MX.at[l, q], MX.at[l, q], s, tp_of(c, p, (q + d) % n)) for d in near]

    def update(l, emit):
        squares = jnp.zeros((tq, LANE), f32)
        for qq in range(n):
            for jp in range(pairs):
                v = MX[l, qq, :, jp * LANE:(jp + 1) * LANE].astype(f32) / PAR[l, qq, jp][5:6]
                squares = squares + v * v
        scale = lax.rsqrt(jnp.sum(squares, axis=1, keepdims=True) * (1.0 / (n * C)) + EPS)
        mixed = jnp.concatenate([MX[l, qq] for qq in range(n)], axis=1)
        for jp in range(pairs):
            w = jnp.concatenate(
                [WO[l, 2 * jp].reshape(n * C, LANE), WO[l, 2 * jp + 1].reshape(n * C, LANE)], axis=1)
            up = jnp.dot(mixed, w, preferred_element_type=f32) * scale
            for j in (0, 1):
                at = tp_of(c, 2 * jp + j, q)
                emit(2 * jp + j, (XM[l, at].astype(f32) + up[:, j * LANE:(j + 1) * LANE]).astype(bf16))

    par_in = [put(PAR.at[:, q], PAR.at[:, q], s, tp_of(c, p, (q + d) % n)) for d in near]
    l1_in = [far_first(1)]
    landed(t_b)
    ring_step(half)
    o_in = [spread_o(0), None]
    norm(0)
    landed(l1_in[0])
    l1_in.append(near_next(1))
    landed_all(WX.at[0, 0:n - 1, :, 0], same)
    landed_all(WX.at[0, :, :, 0], other)
    start = first_half(0)
    x_in = []
    cut = 3 * nt // 4

    def send_x():
        landed(l1_in[1])
        x_in.extend(spread_x(1, 0, cut))

    def send_o():
        o_in[1] = spread_o(1)

    incoming = prefix(0, send_x)
    gathered = second_half(0, start, incoming)
    landed(par_in)
    landed(o_in[0])
    landed(gathered)

    def keep_stream(j, v):
        XM[1, tp_of(c, j, q)] = v

    update(0, keep_stream)
    gathered = []
    for d in near:
        for j in range(n):
            ref = XM.at[1, tp_of(c, j, q)]
            gathered.append(put(ref, ref, s, tp_of(c, p, (q + d) % n)))
    rim1 = next(numbers)
    e, pp = (p + 1) // n, (p + 1) % n
    for j in range(n):
        at = tp_of(c, j, q)
        for qq in range(n):
            put(XM.at[1, at, tq - RIM:tq], XH.at[1, at], (s + e) % ns, tp_of((c + e) % 2, pp, qq), rim1)
    x_in.extend(spread_x(1, cut, nt))
    landed(gathered)
    landed_all(XH.at[1], rim1)
    norm(1)
    landed(x_in)
    start = first_half(1)
    incoming = prefix(1, send_o)
    gathered = second_half(1, start, incoming)
    landed(o_in[1])
    landed(gathered)

    def keep_last(j, v):
        FS[j] = v

    update(1, keep_last)
    last = [put(FS.at[(p + d) % n], OB.at[p], s, tp_of(c, (p + d) % n, q)) for d in near]
    OB[p] = FS[p]
    landed(last)
    for k in range(n):
        out[k * tq:(k + 1) * tq] = OB[k]
    for cp in sent:
        cp.wait_send()
    for cp, k in rim_sends:
        @pl.when(p != k)
        def _():
            cp.wait_send()


def body(tokens, mix_gain, x_weight, gate_weight, conv_taps, a_maps, i_maps, decay_rate, pace, jumps,
         out_gain, out_weight):
    nt = lax.axis_size("tp")
    n = int(round(nt ** 0.5))
    tq = tokens.shape[0] // n
    C = n * HEAD
    D = nt * LANE
    lines = (-1, LANE)
    vmem = pl.BlockSpec(memory_space=pltpu.VMEM)
    xr, orr = x_weight.shape[1], out_weight.shape[1]
    scratch = [
        pltpu.VMEM((LAYERS, xr, LANE), bf16),
        pltpu.VMEM((LAYERS, HEAD, LANE), bf16),
        pltpu.VMEM((LAYERS, ROWS, LANE), f32),
        pltpu.VMEM((2, n * tq, LANE), f32),
        pltpu.VMEM((LAYERS, n, nt, 2, xr, LANE), bf16),
        pltpu.VMEM((LAYERS, n, n, n, 2, orr, LANE), bf16),
        pltpu.VMEM((n, LAYERS, HEAD, LANE), bf16),
        pltpu.VMEM((n, LAYERS, ROWS, LANE), f32),
        pltpu.VMEM((LAYERS, nt, tq, LANE), bf16),
        pltpu.VMEM((LAYERS, nt, RIM, LANE), bf16),
        pltpu.VMEM((RIM + tq, D), bf16),
        pltpu.VMEM((n // 2, RIM + tq, LANE), f32),
        pltpu.VMEM((n // 2, tq, LANE), f32),
        pltpu.VMEM((LAYERS, n // 2, LANE, 2 * LANE), bf16),
        pltpu.VMEM((LAYERS, n, n // 2, ROWS, LANE), f32),
        pltpu.VMEM((n // 2, tq, LANE), f32),
        pltpu.VMEM((n // 2, tq, LANE), f32),
        pltpu.VMEM((n // 2, tq // ROWS, ROWS, LANE), f32),
        pltpu.VMEM((n // 2, tq // ROWS, ROWS, LANE), f32),
        pltpu.VMEM((n // 2, tq, LANE), f32),
        pltpu.VMEM((LAYERS, n, tq, C), bf16),
        pltpu.VMEM((LAYERS, n, 1, LANE), f32),
        pltpu.VMEM((LAYERS, 2, n, n, 1, LANE), f32),
        pltpu.VMEM((LAYERS, n, 1, LANE), f32),
        pltpu.VMEM((LAYERS, nt - 1, n, 1, LANE), f32),
        pltpu.VMEM((n, tq, LANE), bf16),
        pltpu.VMEM((n, tq, LANE), bf16),
        pltpu.SemaphoreType.DMA,
        pltpu.SemaphoreType.DMA((320,)),
    ]
    return pl.pallas_call(
        functools.partial(kernel, n, tq),
        out_shape=jax.ShapeDtypeStruct(tokens.shape, bf16),
        in_specs=[vmem] * 12,
        out_specs=vmem,
        scratch_shapes=scratch,
        compiler_params=pltpu.CompilerParams(collective_id=0, has_side_effects=True, vmem_limit_bytes=56 * 1024 * 1024),
    )(tokens, mix_gain, x_weight, gate_weight, out_weight, conv_taps, a_maps, i_maps, decay_rate, out_gain,
      pace.reshape(lines), jumps.reshape(lines))


def solution(mesh):
    in_specs = (
        P("sp", "tp"),
        P(),
        P(None, "sp", "tp"),
        P(None, "sp", "tp"),
        P(None, None, "tp"),
        P(None, "tp", None, None),
        P(None, "tp", None, None),
        P(None, "tp"),
        P("sp"),
        P("sp"),
        P(None, "tp"),
        P(None, "sp", "tp"),
    )
    return jax.shard_map(body, mesh=mesh, in_specs=in_specs, out_specs=P("sp", "tp"), check_vma=False)
```
